128 devices in a mesh: kv: 32 (over z, y, core), tp: 4 (over x).
Axes of the slice: x: 4, y: 4, z: 4, core: 2. Of those that a mesh axis runs over, the one named last changes fastest.
Arguments:
- tokens: bfloat16 [16384, 2048], P('kv', 'tp'), may hold values from -9 to 9
- w_query: bfloat16 [2048, 1536], P(None, 'tp'), may hold values from -1 to 1
- w_key: bfloat16 [2048, 1536], P(None, 'tp'), may hold values from -1 to 1
- w_value: bfloat16 [2048, 1536], P(None, 'tp'), may hold values from -0.5 to 0.5
- w_out: bfloat16 [1536, 2048], P('tp'), may hold values from -0.15625 to 0.15625
- chosen: int32 [512, 24], P('kv'), may hold values from 0 to 511, as said below
Outputs:
- mixed: bfloat16 [16384, 2048], P(('kv', 'tp'))
The draws below stay inside these ranges and needn't reach their ends.
Inputs may be any that keep to these rules, and one draw needn't show every extreme that they name: `chosen`: row c names blocks no later than c; its first entry is c and its second c - 1 (0 for row 0), and an entry may repeat. Taking the rows in aligned runs of 16, one run for each index of kv, the rows of one run name at most 2 distinct blocks lying in any one other index's positions; in every draw some index of kv names exactly 2 from every earlier index. Every run names some block of the index just before it and of the index half the axis before it, where those exist.
All inputs are finite; a program needn't handle non-finite values.
Results may differ from the reference program's by a relative error of at most 0.014.
Values may be sent and summed in bfloat16 or wider, within the bound.
No kernel may reach another device: no remote copies, remote signals or barrier semaphores. Data moves between devices by JAX's collectives and lax.ppermute only.
A program may use at most 320 MiB of HBM per device.

```python
import math
import jax
import jax.numpy as jnp
from jax import lax

D = 2048
HEADS = 12
HD = 128
BLK = 32
SEL = 24
MOST = 2
TOK_DEV = 512
TOKENS = 16384
N_KV = 32
N_TP = 4


def draw_tokens(key, part):
    base_key = jax.random.fold_in(key, 7)
    first, second, third = jax.random.split(base_key, 3)
    values = jnp.clip(jax.random.normal(first, (TOKENS, D), jnp.float32), -8.0, 8.0)
    return values.astype(jnp.bfloat16)


def weight_pair(key):
    first = jax.random.normal(jax.random.fold_in(key, 101), (D, HEADS * HD), jnp.float32) / math.sqrt(D)
    second = jax.random.normal(jax.random.fold_in(key, 102), (D, HEADS * HD), jnp.float32) / math.sqrt(D)
    return (first, second)


def draw_w_query(key, part):
    first, second = weight_pair(key)
    return jnp.clip(2.0 * first, -1.0, 1.0).astype(jnp.bfloat16)


def draw_w_key(key, part):
    first, second = weight_pair(key)
    values = second
    return jnp.clip(values, -1.0, 1.0).astype(jnp.bfloat16)


def draw_chosen(key, part):
    per_dev = TOK_DEV // BLK
    ndevs = N_KV
    nblocks = per_dev * ndevs
    keys = jax.random.split(jax.random.fold_in(key, 11), 7)
    popular = jnp.maximum(jax.random.randint(keys[0], (nblocks,), 0, 8) - 4, 0)
    noise = jax.random.randint(keys[1], (nblocks,), 0, 4096)
    block_ids = jnp.arange(nblocks, dtype=jnp.int32)
    score = popular * (1 << 24) + noise * 256 + block_ids % per_dev
    devices = jnp.arange(ndevs, dtype=jnp.int32)
    full_dev = jax.random.randint(keys[2], (), 1, ndevs)
    extra_full = jax.random.randint(keys[3], (ndevs,), 0, 4) == 0
    counts = jax.random.randint(keys[4], (ndevs, ndevs), 0, MOST + 1)
    is_full = (devices == full_dev) | extra_full
    counts = jnp.where(is_full[:, None], MOST, counts)
    before = devices[None, :] == devices[:, None] - 1
    halfway = devices[None, :] == devices[:, None] - ndevs // 2
    counts = jnp.where(before | halfway, jnp.maximum(counts, 1), counts)
    counts = jnp.where(devices[None, :] < devices[:, None], counts, 0)
    boost = (block_ids[None, :] == devices[:, None] * per_dev - 1).astype(jnp.int32) * (1 << 30)
    dev_score = (score[None, :] + boost).reshape(ndevs, ndevs, per_dev)
    ranks = jnp.sum((dev_score[:, :, None, :] > dev_score[:, :, :, None]).astype(jnp.int32), axis=-1)
    in_pool = (ranks < counts[:, :, None]).reshape(ndevs, nblocks)
    pool_pos = jnp.cumsum(in_pool.astype(jnp.int32), axis=1) - 1
    pool_size = jnp.sum(in_pool.astype(jnp.int32), axis=1)
    fill_slots = SEL - 2
    places = jnp.arange(fill_slots * per_dev, dtype=jnp.int32)
    hit = in_pool[:, None, :] & (pool_pos[:, None, :] == places[None, :, None])
    elements = jnp.sum(hit.astype(jnp.int32) * block_ids[None, None, :], axis=-1)
    rows_in = jnp.arange(per_dev, dtype=jnp.int32)
    slot_in = jnp.arange(fill_slots, dtype=jnp.int32)
    place_idx = slot_in[None, :] * per_dev + rows_in[:, None]
    random_pick = jax.random.randint(keys[5], (ndevs, per_dev, fill_slots), 0, 1 << 20)
    safe_size = jnp.maximum(pool_size, 1)[:, None, None]
    take = jnp.where(place_idx[None] < pool_size[:, None, None], place_idx[None], random_pick % safe_size)
    picked = jnp.take_along_axis(elements, take.reshape(ndevs, -1), axis=1).reshape(ndevs, per_dev, fill_slots)
    own_block = devices[:, None] * per_dev + rows_in[None, :]
    own_fill = devices[:, None, None] * per_dev + random_pick % (rows_in[None, :, None] + 1)
    filled = jnp.where(pool_size[:, None, None] > 0, picked, own_fill)
    prev_block = jnp.maximum(own_block - 1, 0)
    rows = jnp.concatenate([own_block[:, :, None], prev_block[:, :, None], filled], axis=-1)
    return rows.reshape(nblocks, SEL).astype(jnp.int32)


def steps_of(rng, dims, cuts, low, top_value):
    def one(axis_at, parts):
        steps = jax.random.uniform(jax.random.fold_in(jax.random.fold_in(rng, 6), axis_at), (parts,), jnp.float32, low / len(cuts), top_value / len(cuts))
        return jnp.repeat(jnp.exp(steps), dims[axis_at] // parts).reshape((-1,) + (1,) * (len(dims) - axis_at - 1))

    gain = one(*cuts[0])
    for cut in cuts[1:]:
        gain = gain * one(*cut)
    return gain


def gaussian(rng, extent, width, limit, cuts=(), kind=jnp.bfloat16):
    gain = steps_of(rng, extent, cuts, -0.22, 0.18) if cuts else 1.0
    values = jax.random.normal(rng, extent, jnp.float32) * width * gain
    return jnp.minimum(jnp.maximum(values, -limit), limit).astype(kind)


def setup_inputs(seed: int = 0) -> dict:
    key_of = jax.random.split(jax.random.key(seed), 7)
    tokens = draw_tokens(jax.random.fold_in(key_of[6], 71), 0)
    w_query = draw_w_query(jax.random.fold_in(key_of[6], 71), 0)
    w_key = draw_w_key(jax.random.fold_in(key_of[6], 71), 0)
    w_value = gaussian(key_of[3], (D, HEADS * HD), (D // 16) ** -0.5, 0.5, ((1, 4),))
    w_out = gaussian(key_of[4], (HEADS * HD, D), (HEADS * HD) ** -0.5, 0.15625, ((0, 4),))
    chosen = draw_chosen(jax.random.fold_in(key_of[6], 71), 0)
    return {"tokens": tokens, "w_query": w_query, "w_key": w_key, "w_value": w_value, "w_out": w_out, "chosen": chosen}


NEG = -1e30


def reference(tokens, w_query, w_key, w_value, w_out, chosen):
    query_rows = jnp.dot(tokens, w_query, preferred_element_type=jnp.float32).astype(jnp.bfloat16)
    key_rows = jnp.dot(tokens, w_key, preferred_element_type=jnp.float32).astype(jnp.bfloat16)
    value_rows = jnp.dot(tokens, w_value, preferred_element_type=jnp.float32).astype(jnp.bfloat16)
    total_rows = tokens.shape[0]
    block_count = total_rows // BLK
    query_blocks = query_rows.reshape(block_count, BLK, HEADS, HD)
    key_blocks = key_rows.reshape(block_count, BLK, HEADS, HD)
    value_blocks = value_rows.reshape(block_count, BLK, HEADS, HD)
    offsets = jnp.arange(BLK, dtype=jnp.int32)
    slot_ids = jnp.arange(SEL, dtype=jnp.int32)
    earlier_slot = slot_ids[None, :] < slot_ids[:, None]

    def one_block(packed):
        query_block, chosen_row, block_index = packed
        repeat_slot = jnp.any((chosen_row[:, None] == chosen_row[None, :]) & earlier_slot, axis=1)
        gathered_keys = key_blocks[chosen_row].astype(jnp.float32)
        gathered_values = value_blocks[chosen_row].astype(jnp.float32)
        scores = jnp.einsum('qhd,jkhd->hqjk', query_block.astype(jnp.float32), gathered_keys) * (HD ** -0.5)
        key_pos = chosen_row[:, None] * BLK + offsets[None, :]
        query_pos = block_index * BLK + offsets
        allowed = (~repeat_slot)[None, :, None] & (key_pos[None, :, :] <= query_pos[:, None, None])
        scores = jnp.where(allowed[None], scores, NEG)
        weights = jax.nn.softmax(scores.reshape(HEADS, BLK, SEL * BLK), axis=-1).reshape(HEADS, BLK, SEL, BLK)
        mixed_heads = jnp.einsum('hqjk,jkhd->qhd', weights, gathered_values)
        return mixed_heads.astype(jnp.bfloat16).reshape(BLK, HEADS * HD)

    attended = lax.map(one_block, (query_blocks, chosen, jnp.arange(block_count, dtype=jnp.int32)))
    attended = attended.reshape(total_rows, HEADS * HD)
    group_width = HEADS * HD // N_TP
    summed = jnp.zeros((total_rows, w_out.shape[1]), jnp.float32)
    for group in range(N_TP):
        partial_value = jnp.dot(attended[:, group * group_width:(group + 1) * group_width],
                          w_out[group * group_width:(group + 1) * group_width],
                          preferred_element_type=jnp.float32).astype(jnp.bfloat16)
        partial_value = lax.optimization_barrier(partial_value)
        summed = summed + partial_value.astype(jnp.float32)
    return summed.astype(jnp.bfloat16)
```

```python
import jax
import jax.numpy as jnp
from jax import lax
from jax.experimental import pallas as pl
from jax.experimental.pallas import tpu as pltpu
from jax.sharding import Mesh
from jax.sharding import PartitionSpec as P

HD = 128
BLK = 32
MOST = 2
KV = ("kv_0", "kv_1", "kv_2")
KV_TP = ("kv_0", "kv_1", "kv_2", "tp")
NEG = -1e30
LOG2E = 1.4426950408889634
VMEM_LIMIT = 24 * 1024 * 1024


def params(dims=None):
    return pltpu.CompilerParams(vmem_limit_bytes=VMEM_LIMIT, dimension_semantics=dims)


def cost(flops, nbytes, exps=0):
    return pl.CostEstimate(flops=int(flops), bytes_accessed=int(nbytes), transcendentals=int(exps))


def f32dot(a, b):
    return jnp.dot(a, b, preferred_element_type=jnp.float32)


def shifted(array, axis, by):
    count = lax.axis_size(axis)
    return lax.ppermute(array, axis, [(i, (i + by) % count) for i in range(count)])


def project_first(where, tokens, w_key, w_value):
    rows, feat = tokens.shape
    width = w_key.shape[1]

    def body(where_ref, tok_ref, wk_ref, wv_ref, out_ref):
        out_ref[:, :width] = f32dot(tok_ref[...], wk_ref[...])
        out_ref[:, width:] = f32dot(tok_ref[...], wv_ref[...])

    chunk = pl.BlockSpec((feat, width), lambda i, s: (s[0], 0))
    return pl.pallas_call(
        body,
        grid_spec=pltpu.PrefetchScalarGridSpec(
            num_scalar_prefetch=1,
            grid=(1,),
            in_specs=[pl.BlockSpec((rows, feat), lambda i, s: (0, 0)), chunk, chunk],
            out_specs=pl.BlockSpec((rows, 2 * width), lambda i, s: (0, 0)),
        ),
        out_shape=jax.ShapeDtypeStruct((rows, 2 * width), jnp.float32),
        compiler_params=params(),
        cost_estimate=cost(4 * rows * feat * width, 6 * feat * width),
        name="project_first",
    )(where, tokens, w_key, w_value)


def project_sides(where, left, right, w_key, w_value, total):
    rows, feat = left.shape
    width = w_key.shape[1]

    def body(where_ref, l_ref, r_ref, wkl, wkr, wvl, wvr, tot_ref, out_ref):
        out_ref[:, :width] = tot_ref[:, :width] + f32dot(l_ref[...], wkl[...]) + f32dot(r_ref[...], wkr[...])
        out_ref[:, width:] = tot_ref[:, width:] + f32dot(l_ref[...], wvl[...]) + f32dot(r_ref[...], wvr[...])

    left_chunk = pl.BlockSpec((feat, width), lambda i, s: (s[1], 0))
    right_chunk = pl.BlockSpec((feat, width), lambda i, s: (s[2], 0))
    toks = pl.BlockSpec((rows, feat), lambda i, s: (0, 0))
    whole = pl.BlockSpec((rows, 2 * width), lambda i, s: (0, 0))
    return pl.pallas_call(
        body,
        grid_spec=pltpu.PrefetchScalarGridSpec(
            num_scalar_prefetch=1,
            grid=(1,),
            in_specs=[toks, toks, left_chunk, right_chunk, left_chunk, right_chunk, whole],
            out_specs=whole,
        ),
        out_shape=jax.ShapeDtypeStruct((rows, 2 * width), jnp.float32),
        compiler_params=params(),
        cost_estimate=cost(8 * rows * feat * width, 12 * feat * width),
        name="project_sides",
    )(where, left, right, w_key, w_key, w_value, w_value, total)


def project_last(where, picked, top, bottom, w_key, w_value, total):
    half, feat = top.shape
    rows = 2 * half
    width = w_key.shape[1]
    slots = picked.shape[0]

    def body(where_ref, pick_ref, t_ref, b_ref, wk, wv, tot_ref, out_ref, send_ref):
        for lo, ref in ((0, t_ref), (half, b_ref)):
            span = slice(lo, lo + half)
            out_ref[span, :width] = (tot_ref[span, :width] + f32dot(ref[...], wk[...])).astype(jnp.bfloat16)
            out_ref[span, width:] = (tot_ref[span, width:] + f32dot(ref[...], wv[...])).astype(jnp.bfloat16)
        for i in range(slots):
            start = pl.multiple_of(pick_ref[i] * BLK, BLK)
            send_ref[i] = out_ref[pl.ds(start, BLK), :]

    chunk = pl.BlockSpec((feat, width), lambda i, s, p: (s[3], 0))
    toks = pl.BlockSpec((half, feat), lambda i, s, p: (0, 0))
    whole = pl.BlockSpec((rows, 2 * width), lambda i, s, p: (0, 0))
    return pl.pallas_call(
        body,
        grid_spec=pltpu.PrefetchScalarGridSpec(
            num_scalar_prefetch=2,
            grid=(1,),
            in_specs=[toks, toks, chunk, chunk, whole],
            out_specs=[whole, pl.BlockSpec((slots, BLK, 2 * width), lambda i, s, p: (0, 0, 0))],
        ),
        out_shape=[
            jax.ShapeDtypeStruct((rows, 2 * width), jnp.bfloat16),
            jax.ShapeDtypeStruct((slots, BLK, 2 * width), jnp.bfloat16),
        ],
        compiler_params=params(),
        cost_estimate=cost(4 * rows * feat * width, 12 * feat * width),
        name="project_last",
    )(where, picked, top, bottom, w_key, w_value, total)


def project_query(where, own, left, right, top, bottom, w_query):
    rows, feat = own.shape
    half = top.shape[0]
    width = w_query.shape[1]

    def body(where_ref, o_ref, l_ref, r_ref, t_ref, b_ref, wo, wl, wr, wf, out_ref):
        for lo, far in ((0, t_ref), (half, b_ref)):
            span = slice(lo, lo + half)
            total = f32dot(o_ref[span, :], wo[...]) + f32dot(l_ref[span, :], wl[...])
            total = total + f32dot(r_ref[span, :], wr[...]) + f32dot(far[...], wf[...])
            out_ref[span, :] = total.astype(jnp.bfloat16)

    def chunk(k):
        return pl.BlockSpec((feat, width), lambda i, s: (s[k], 0))

    toks = pl.BlockSpec((rows, feat), lambda i, s: (0, 0))
    halves = pl.BlockSpec((half, feat), lambda i, s: (0, 0))
    return pl.pallas_call(
        body,
        grid_spec=pltpu.PrefetchScalarGridSpec(
            num_scalar_prefetch=1,
            grid=(1,),
            in_specs=[toks, toks, toks, halves, halves, chunk(0), chunk(1), chunk(2), chunk(3)],
            out_specs=pl.BlockSpec((rows, width), lambda i, s: (0, 0)),
        ),
        out_shape=jax.ShapeDtypeStruct((rows, width), jnp.bfloat16),
        compiler_params=params(),
        cost_estimate=cost(8 * rows * feat * width, 16 * feat * width),
        name="project_query",
    )(where, own, left, right, top, bottom, w_query, w_query, w_query, w_query)


def masks(ids, chosen_cols):
    slots = ids.shape[0]
    wide, lanes = chosen_cols.shape

    def body(ids_ref, cho_ref, out_ref):
        cols = cho_ref[...]
        for i in range(slots):
            hit = jnp.max((cols == ids_ref[i]).astype(jnp.int32), axis=0, keepdims=True)
            row = jnp.where(hit > 0, 0.0, NEG)
            out_ref[i * BLK : (i + 1) * BLK, :] = jnp.broadcast_to(row, (BLK, lanes)).astype(jnp.bfloat16)

    return pl.pallas_call(
        body,
        grid_spec=pltpu.PrefetchScalarGridSpec(
            num_scalar_prefetch=1,
            grid=(1,),
            in_specs=[pl.BlockSpec((wide, lanes), lambda i, s: (0, 0))],
            out_specs=pl.BlockSpec((slots * BLK, lanes), lambda i, s: (0, 0)),
        ),
        out_shape=jax.ShapeDtypeStruct((slots * BLK, lanes), jnp.bfloat16),
        compiler_params=params(),
        cost_estimate=cost(slots * wide * lanes, slots * BLK * lanes * 2),
        name="masks",
    )(ids, chosen_cols)


def widened(query, first_row):
    rows = query.shape[0]
    block = (lax.broadcasted_iota(jnp.int32, (rows, HD), 0) + first_row) // BLK
    lane = lax.broadcasted_iota(jnp.int32, (rows, HD), 1)
    return jnp.concatenate([query, (block == lane).astype(jnp.bfloat16)], axis=1)


def scores_of(query, keys):
    return lax.dot_general(query, keys, (((1,), (1,)), ((), ())), preferred_element_type=jnp.float32)


def attend_own(query, pair, mask):
    rows, width = query.shape
    heads = width // HD
    scale = HD ** (-0.5) * LOG2E
    tile = 256

    def body(q_ref, k_ref, v_ref, mask_ref, high_ref, tot_ref, sum_ref):
        keys = jnp.concatenate([k_ref[...], mask_ref[...]], axis=1)
        values = jnp.concatenate([v_ref[...], jnp.ones_like(v_ref)], axis=1)
        for lo in range(0, rows, tile):
            span = slice(lo, lo + tile)
            count = lo + tile
            scores = scores_of(widened(q_ref[span, :], lo), keys[:count])
            row = lax.broadcasted_iota(jnp.int32, scores.shape, 0) + lo
            col = lax.broadcasted_iota(jnp.int32, scores.shape, 1)
            scores = jnp.where(col <= row, scores, NEG)
            high = jnp.max(scores, axis=1, keepdims=True)
            weights = jnp.exp2((scores - high) * scale).astype(jnp.bfloat16)
            summed = f32dot(weights, values[:count])
            high_ref[span, :] = jnp.broadcast_to(high, (tile, HD))
            tot_ref[span, :] = summed[:, HD:]
            sum_ref[span, :] = summed[:, :HD]

    column = pl.BlockSpec((rows, HD), lambda h: (0, h))
    return pl.pallas_call(
        body,
        grid=(heads,),
        in_specs=[
            column,
            column,
            pl.BlockSpec((rows, HD), lambda h: (0, heads + h)),
            pl.BlockSpec((rows, HD), lambda h: (0, 0)),
        ],
        out_specs=[column, column, column],
        out_shape=[jax.ShapeDtypeStruct((rows, width), jnp.float32)] * 3,
        compiler_params=params(("arbitrary",)),
        cost_estimate=cost(8 * rows * rows * width, 16 * rows * width, rows * rows * heads),
        name="attend_own",
    )(query, pair, pair, mask)


def attend_far(query, got, mask, high, total, summed):
    rows, width = query.shape
    heads = width // HD
    count = got.shape[0]
    scale = HD ** (-0.5) * LOG2E
    tile = 128

    def body(q_ref, k_ref, v_ref, mask_ref, high_ref, tot_ref, sum_ref, out_ref, keys, values):
        keys[:, :HD] = k_ref[...]
        keys[:, HD:] = mask_ref[...]
        values[:, :HD] = v_ref[...]
        values[:, HD:] = jnp.ones_like(v_ref)
        for lo in range(0, rows, tile):
            span = slice(lo, lo + tile)
            scores = scores_of(widened(q_ref[span, :], lo), keys[...])
            own = high_ref[span, :]
            top = jnp.maximum(jnp.max(scores, axis=1, keepdims=True), own[:, :1])
            weights = jnp.exp2((scores - top) * scale).astype(jnp.bfloat16)
            far = f32dot(weights, values[...])
            keep = jnp.exp2((own - top) * scale)
            result = (far[:, :HD] + keep * sum_ref[span, :]) / (far[:, HD:] + keep * tot_ref[span, :])
            out_ref[span, :] = result.astype(jnp.bfloat16)

    column = pl.BlockSpec((rows, HD), lambda h: (0, h))
    return pl.pallas_call(
        body,
        grid=(heads,),
        in_specs=[
            column,
            pl.BlockSpec((count, HD), lambda h: (0, h)),
            pl.BlockSpec((count, HD), lambda h: (0, heads + h)),
            pl.BlockSpec((count, HD), lambda h: (0, 0)),
            column,
            column,
            column,
        ],
        out_specs=column,
        out_shape=jax.ShapeDtypeStruct((rows, width), jnp.bfloat16),
        scratch_shapes=[pltpu.VMEM((count, 2 * HD), jnp.bfloat16)] * 2,
        compiler_params=params(("arbitrary",)),
        cost_estimate=cost(8 * rows * count * width, 4 * count * width, rows * count * heads),
        name="attend_far",
    )(query, got, got, mask, high, total, summed)


def requests(chosen, my_index, peers, per_dev):
    block_total = peers * per_dev
    wanted = jnp.any(
        chosen[:, :, None] == jnp.arange(block_total, dtype=jnp.int32)[None, None, :], axis=(0, 1)
    )
    peer_ids = jnp.arange(peers, dtype=jnp.int32)
    wanted = wanted.reshape(peers, per_dev) & (peer_ids != my_index)[:, None]
    local_ids = jnp.arange(per_dev, dtype=jnp.int32)[None, :]
    first = jnp.min(jnp.where(wanted, local_ids, per_dev), axis=1)
    last = jnp.max(jnp.where(wanted, local_ids, -1), axis=1)
    return jnp.stack([jnp.where(first < per_dev, first, -1), jnp.where(last > first, last, -1)], axis=1)


def local(tokens, w_query, w_key, w_value, w_out, chosen):
    tok_rows = tokens.shape[0]
    width = w_query.shape[1]
    half = tok_rows // 2
    per_dev = tok_rows // BLK
    peers = lax.axis_size(KV)
    my_index = lax.axis_index(KV)
    first_block = my_index * per_dev
    tp = lax.axis_index("tp")
    count = lax.axis_size("tp")

    left = shifted(tokens, "tp", 1)
    right = shifted(tokens, "tp", -1)
    where = jnp.stack([tp, (tp + count - 1) % count, (tp + 1) % count, (tp + 2) % count]).astype(jnp.int32)

    request = requests(chosen, my_index, peers, per_dev)
    asked = lax.all_to_all(request, KV, 0, 0, tiled=True)
    picked = jnp.clip(asked, 0).reshape(-1)

    total = project_first(where, tokens, w_key, w_value)
    top = shifted(left[:half], "tp", 1)
    bottom = shifted(right[half:], "tp", -1)
    total = project_sides(where, left, right, w_key, w_value, total)
    pair, send = project_last(where, picked, top, bottom, w_key, w_value, total)
    got = lax.all_to_all(send, KV, split_axis=0, concat_axis=0, tiled=True)

    query = project_query(where, tokens, left, right, top, bottom, w_query)
    peer_base = jnp.arange(peers, dtype=jnp.int32)[:, None] * per_dev
    got_ids = jnp.where(request >= 0, peer_base + request, -1).reshape(-1)
    own_ids = first_block + jnp.arange(per_dev, dtype=jnp.int32)
    cols = jnp.pad(chosen.T, ((0, 0), (0, HD - per_dev)), constant_values=-2)
    mask = masks(jnp.concatenate([own_ids, got_ids]), cols)
    high, totals, summed = attend_own(query, pair, mask[:tok_rows])
    attended = attend_far(query, got.reshape(-1, 2 * width), mask[tok_rows:], high, totals, summed)

    partial = f32dot(attended, w_out).astype(jnp.bfloat16)
    parts = lax.all_to_all(partial.reshape(count, tok_rows // count, -1), "tp", 0, 0, tiled=True)
    return jnp.sum(parts.astype(jnp.float32), axis=0).astype(jnp.bfloat16)


def solution(mesh):
    finer = Mesh(mesh.devices.reshape(4, 4, 2, mesh.shape["tp"]), ("kv_0", "kv_1", "kv_2", "tp"))
    placed = (P(KV, "tp"), P(None, "tp"), P(None, "tp"), P(None, "tp"), P("tp", None), P(KV, None))
    return jax.shard_map(
        local, mesh=finer, in_specs=placed, out_specs=P(KV_TP, None), check_vma=False
    )
```

```python
import jax
import jax.numpy as jnp
from jax import lax
from jax.experimental import pallas as pl
from jax.experimental.pallas import tpu as pltpu
from jax.sharding import Mesh
from jax.sharding import PartitionSpec as P

HD = 128
BLK = 32
MOST = 2
KV = ("kv_0", "kv_1", "kv_2")
KV_TP = ("kv_0", "kv_1", "kv_2", "tp")
NEG = -1e30
LOG2E = 1.4426950408889634
VMEM_LIMIT = 24 * 1024 * 1024


def params(dims=None):
    return pltpu.CompilerParams(vmem_limit_bytes=VMEM_LIMIT, dimension_semantics=dims)


def cost(flops, nbytes, exps=0):
    return pl.CostEstimate(flops=int(flops), bytes_accessed=int(nbytes), transcendentals=int(exps))


def f32dot(a, b):
    return jnp.dot(a, b, preferred_element_type=jnp.float32)


def shifted(array, axis, by):
    count = lax.axis_size(axis)
    return lax.ppermute(array, axis, [(i, (i + by) % count) for i in range(count)])


def plan(my_index, chosen, peers):
    rows, wide = chosen.shape
    slots = peers * MOST

    def body(me_ref, cho_ref, req_ref, mask_ref):
        me = me_ref[0]
        entries = cho_ref[...]
        peer = lax.broadcasted_iota(jnp.int32, (peers, wide), 0)
        low = jnp.full((peers, wide), rows, jnp.int32)
        high = jnp.full((peers, wide), -1, jnp.int32)
        for r in range(rows):
            entry = jnp.broadcast_to(entries[r : r + 1, :], (peers, wide))
            block = entry - peer * rows
            mine = (block >= 0) & (block < rows)
            low = jnp.where(mine, jnp.minimum(low, block), low)
            high = jnp.where(mine, jnp.maximum(high, block), high)
        low = jnp.min(low, axis=1, keepdims=True)
        high = jnp.max(high, axis=1, keepdims=True)
        far = lax.broadcasted_iota(jnp.int32, (peers, 1), 0) != me
        first = jnp.where(far & (low < rows), low, -1)
        second = jnp.where(far & (high > low), high, -1)
        lane = lax.broadcasted_iota(jnp.int32, (peers, HD), 1)
        req_ref[...] = jnp.where(lane == 0, first, jnp.where(lane == 1, second, -1))
        at = lax.broadcasted_iota(jnp.int32, (peers, HD), 0)
        named = jnp.where(lane == MOST * at, first, jnp.where(lane == MOST * at + 1, second, -1))
        named = jnp.where(named >= 0, named + at * rows, -1)
        ids = jnp.max(named, axis=0, keepdims=True)
        slot = lax.broadcasted_iota(jnp.int32, (1, HD), 1)
        own = (slot >= slots) & (slot < slots + rows)
        ids = jnp.where(own, me * rows + slot - slots, ids)
        seen = entries[:, :1] == ids
        for k in range(1, wide):
            seen = seen | (entries[:, k : k + 1] == ids)
        bias = jnp.where(seen, 0.0, NEG)
        for r in range(rows):
            mask_ref[r * BLK : (r + 1) * BLK, :] = jnp.broadcast_to(bias[r : r + 1, :], (BLK, HD)).astype(jnp.bfloat16)

    return pl.pallas_call(
        body,
        grid_spec=pltpu.PrefetchScalarGridSpec(
            num_scalar_prefetch=1,
            grid=(1,),
            in_specs=[pl.BlockSpec((rows, wide), lambda i, s: (0, 0))],
            out_specs=[
                pl.BlockSpec((peers, HD), lambda i, s: (0, 0)),
                pl.BlockSpec((rows * BLK, HD), lambda i, s: (0, 0)),
            ],
        ),
        out_shape=[
            jax.ShapeDtypeStruct((peers, HD), jnp.int32),
            jax.ShapeDtypeStruct((rows * BLK, HD), jnp.bfloat16),
        ],
        compiler_params=params(),
        cost_estimate=cost(1000000, 200000),
        name="plan",
    )(my_index, chosen)


def project_first(where, tokens, w_key, w_value):
    rows, feat = tokens.shape
    width = w_key.shape[1]

    def body(where_ref, tok_ref, wk_ref, wv_ref, out_ref):
        out_ref[:, :width] = f32dot(tok_ref[...], wk_ref[...])
        out_ref[:, width:] = f32dot(tok_ref[...], wv_ref[...])

    chunk = pl.BlockSpec((feat, width), lambda i, s: (s[0], 0))
    return pl.pallas_call(
        body,
        grid_spec=pltpu.PrefetchScalarGridSpec(
            num_scalar_prefetch=1,
            grid=(1,),
            in_specs=[pl.BlockSpec((rows, feat), lambda i, s: (0, 0)), chunk, chunk],
            out_specs=pl.BlockSpec((rows, 2 * width), lambda i, s: (0, 0)),
        ),
        out_shape=jax.ShapeDtypeStruct((rows, 2 * width), jnp.float32),
        compiler_params=params(),
        cost_estimate=cost(4 * rows * feat * width, 6 * feat * width),
        name="project_first",
    )(where, tokens, w_key, w_value)


def project_sides(where, left, right, w_key, w_value, total):
    rows, feat = left.shape
    width = w_key.shape[1]

    def body(where_ref, l_ref, r_ref, wkl, wkr, wvl, wvr, tot_ref, out_ref):
        out_ref[:, :width] = tot_ref[:, :width] + f32dot(l_ref[...], wkl[...]) + f32dot(r_ref[...], wkr[...])
        out_ref[:, width:] = tot_ref[:, width:] + f32dot(l_ref[...], wvl[...]) + f32dot(r_ref[...], wvr[...])

    left_chunk = pl.BlockSpec((feat, width), lambda i, s: (s[1], 0))
    right_chunk = pl.BlockSpec((feat, width), lambda i, s: (s[2], 0))
    toks = pl.BlockSpec((rows, feat), lambda i, s: (0, 0))
    whole = pl.BlockSpec((rows, 2 * width), lambda i, s: (0, 0))
    return pl.pallas_call(
        body,
        grid_spec=pltpu.PrefetchScalarGridSpec(
            num_scalar_prefetch=1,
            grid=(1,),
            in_specs=[toks, toks, left_chunk, right_chunk, left_chunk, right_chunk, whole],
            out_specs=whole,
        ),
        out_shape=jax.ShapeDtypeStruct((rows, 2 * width), jnp.float32),
        compiler_params=params(),
        cost_estimate=cost(8 * rows * feat * width, 12 * feat * width),
        name="project_sides",
    )(where, left, right, w_key, w_key, w_value, w_value, total)


def project_last(where, picked, top, bottom, w_key, w_value, total):
    half, feat = top.shape
    rows = 2 * half
    width = w_key.shape[1]
    slots = picked.shape[0] * MOST

    def body(where_ref, pick_ref, t_ref, b_ref, wk, wv, tot_ref, out_ref, send_ref):
        for lo, ref in ((0, t_ref), (half, b_ref)):
            span = slice(lo, lo + half)
            out_ref[span, :width] = (tot_ref[span, :width] + f32dot(ref[...], wk[...])).astype(jnp.bfloat16)
            out_ref[span, width:] = (tot_ref[span, width:] + f32dot(ref[...], wv[...])).astype(jnp.bfloat16)
        for i in range(slots):
            block = jnp.maximum(pick_ref[i // MOST, i % MOST], 0)
            send_ref[i] = out_ref[pl.ds(pl.multiple_of(block * BLK, BLK), BLK), :]

    chunk = pl.BlockSpec((feat, width), lambda i, s, p: (s[3], 0))
    toks = pl.BlockSpec((half, feat), lambda i, s, p: (0, 0))
    whole = pl.BlockSpec((rows, 2 * width), lambda i, s, p: (0, 0))
    return pl.pallas_call(
        body,
        grid_spec=pltpu.PrefetchScalarGridSpec(
            num_scalar_prefetch=2,
            grid=(1,),
            in_specs=[toks, toks, chunk, chunk, whole],
            out_specs=[whole, pl.BlockSpec((slots, BLK, 2 * width), lambda i, s, p: (0, 0, 0))],
        ),
        out_shape=[
            jax.ShapeDtypeStruct((rows, 2 * width), jnp.bfloat16),
            jax.ShapeDtypeStruct((slots, BLK, 2 * width), jnp.bfloat16),
        ],
        compiler_params=params(),
        cost_estimate=cost(4 * rows * feat * width, 12 * feat * width),
        name="project_last",
    )(where, picked, top, bottom, w_key, w_value, total)


def project_query(where, own, left, right, top, bottom, w_query):
    rows, feat = own.shape
    half = top.shape[0]
    width = w_query.shape[1]

    def body(where_ref, o_ref, l_ref, r_ref, t_ref, b_ref, wo, wl, wr, wf, out_ref):
        for lo, far in ((0, t_ref), (half, b_ref)):
            span = slice(lo, lo + half)
            total = f32dot(o_ref[span, :], wo[...]) + f32dot(l_ref[span, :], wl[...])
            total = total + f32dot(r_ref[span, :], wr[...]) + f32dot(far[...], wf[...])
            out_ref[span, :] = total.astype(jnp.bfloat16)

    def chunk(k):
        return pl.BlockSpec((feat, width), lambda i, s: (s[k], 0))

    toks = pl.BlockSpec((rows, feat), lambda i, s: (0, 0))
    halves = pl.BlockSpec((half, feat), lambda i, s: (0, 0))
    return pl.pallas_call(
        body,
        grid_spec=pltpu.PrefetchScalarGridSpec(
            num_scalar_prefetch=1,
            grid=(1,),
            in_specs=[toks, toks, toks, halves, halves, chunk(0), chunk(1), chunk(2), chunk(3)],
            out_specs=pl.BlockSpec((rows, width), lambda i, s: (0, 0)),
        ),
        out_shape=jax.ShapeDtypeStruct((rows, width), jnp.bfloat16),
        compiler_params=params(),
        cost_estimate=cost(8 * rows * feat * width, 16 * feat * width),
        name="project_query",
    )(where, own, left, right, top, bottom, w_query, w_query, w_query, w_query)


def one_hot(rows, first_slot):
    slot = lax.broadcasted_iota(jnp.int32, (rows, HD), 0) // BLK + first_slot
    return (slot == lax.broadcasted_iota(jnp.int32, (rows, HD), 1)).astype(jnp.bfloat16)


def scores_of(query, keys):
    return lax.dot_general(query, keys, (((1,), (1,)), ((), ())), preferred_element_type=jnp.float32)


def attend_own(query, pair, mask, first_slot):
    rows, width = query.shape
    heads = width // HD
    scale = HD ** (-0.5) * LOG2E
    tile = 256

    def body(q_ref, k_ref, v_ref, mask_ref, high_ref, tot_ref, sum_ref):
        keys = jnp.concatenate([k_ref[...], one_hot(rows, first_slot)], axis=1)
        values = jnp.concatenate([v_ref[...], jnp.ones_like(v_ref)], axis=1)
        for lo in range(0, rows, tile):
            span = slice(lo, lo + tile)
            count = lo + tile
            wide = jnp.concatenate([q_ref[span, :], mask_ref[span, :]], axis=1)
            scores = scores_of(wide, keys[:count])
            row = lax.broadcasted_iota(jnp.int32, scores.shape, 0) + lo
            col = lax.broadcasted_iota(jnp.int32, scores.shape, 1)
            scores = jnp.where(col <= row, scores, NEG)
            high = jnp.max(scores, axis=1, keepdims=True)
            weights = jnp.exp2((scores - high) * scale).astype(jnp.bfloat16)
            summed = f32dot(weights, values[:count])
            high_ref[span, :] = jnp.broadcast_to(high, (tile, HD))
            tot_ref[span, :] = summed[:, HD:]
            sum_ref[span, :] = summed[:, :HD]

    column = pl.BlockSpec((rows, HD), lambda h: (0, h))
    return pl.pallas_call(
        body,
        grid=(heads,),
        in_specs=[
            column,
            column,
            pl.BlockSpec((rows, HD), lambda h: (0, heads + h)),
            pl.BlockSpec((rows, HD), lambda h: (0, 0)),
        ],
        out_specs=[column, column, column],
        out_shape=[jax.ShapeDtypeStruct((rows, width), jnp.float32)] * 3,
        compiler_params=params(("arbitrary",)),
        cost_estimate=cost(8 * rows * rows * width, 16 * rows * width, rows * rows * heads),
        name="attend_own",
    )(query, pair, pair, mask)


def attend_far(where, query, got, mask, high, total, summed):
    rows, width = query.shape
    heads = width // HD
    count = got.shape[0]
    scale = HD ** (-0.5) * LOG2E
    parts = where.shape[0]
    tile = rows // parts
    order = (3, 1, 2, 0)

    def body(where_ref, q_ref, k_ref, v_ref, mask_ref, high_ref, tot_ref, sum_ref, *rest):
        outs, keys, values = rest[:parts], rest[parts], rest[parts + 1]

        @pl.when(pl.program_id(0) == 0)
        def _():
            keys[:, HD:] = one_hot(count, 0)
            values[:, HD:] = jnp.ones_like(v_ref)

        keys[:, :HD] = k_ref[...]
        values[:, :HD] = v_ref[...]

        def scores_at(part):
            span = pl.ds(pl.multiple_of(where_ref[part] * tile, tile), tile)
            wide = jnp.concatenate([q_ref[span, :], mask_ref[span, :]], axis=1)
            return span, scores_of(wide, keys[...])

        later = scores_at(order[0])
        for i, part in enumerate(order):
            span, scores = later
            if i + 1 < parts:
                later = scores_at(order[i + 1])
            own = high_ref[span, :]
            top = jnp.maximum(jnp.max(scores, axis=1, keepdims=True), own[:, :1])
            weights = jnp.exp2((scores - top) * scale).astype(jnp.bfloat16)
            far = f32dot(weights, values[...])
            keep = jnp.exp2((own - top) * scale)
            result = (far[:, :HD] + keep * sum_ref[span, :]) / (far[:, HD:] + keep * tot_ref[span, :])
            outs[part][...] = result.astype(jnp.bfloat16)

    column = pl.BlockSpec((rows, HD), lambda h, s: (0, h))
    return pl.pallas_call(
        body,
        grid_spec=pltpu.PrefetchScalarGridSpec(
            num_scalar_prefetch=1,
            grid=(heads,),
            in_specs=[
                column,
                pl.BlockSpec((count, HD), lambda h, s: (0, h)),
                pl.BlockSpec((count, HD), lambda h, s: (0, heads + h)),
                pl.BlockSpec((rows, HD), lambda h, s: (0, 0)),
                column,
                column,
                column,
            ],
            out_specs=[pl.BlockSpec((tile, HD), lambda h, s: (0, h))] * parts,
            scratch_shapes=[pltpu.VMEM((count, 2 * HD), jnp.bfloat16)] * 2,
        ),
        out_shape=[jax.ShapeDtypeStruct((tile, width), jnp.bfloat16)] * parts,
        compiler_params=params(("arbitrary",)),
        cost_estimate=cost(8 * rows * count * width, 4 * count * width, rows * count * heads),
        name="attend_far",
    )(where, query, got, got, mask, high, total, summed)


def mix(core, attended, w_own, mine, other):
    rows, width = attended[0].shape
    span = mine[0].shape[1]
    part = mine[2].shape[1]

    def body(core_ref, own_ref, l_ref, r_ref, f_ref, w_ref, *rest):
        out_ref = rest[-1]
        for which, pieces in ((core_ref[0], rest[:4]), (1 - core_ref[0], rest[4:8])):
            at = pl.multiple_of(which * span, span)
            total = f32dot(own_ref[...], w_ref[:, pl.ds(at, span)])
            total = total + f32dot(l_ref[...], pieces[0][...]) + f32dot(r_ref[...], pieces[1][...])
            low = total[:, :part] + f32dot(f_ref[...], pieces[2][...])
            high = total[:, part:] + f32dot(f_ref[...], pieces[3][...])
            out_ref[:, pl.ds(at, part)] = low.astype(jnp.bfloat16)
            out_ref[:, pl.ds(at + part, part)] = high.astype(jnp.bfloat16)

    def whole(array):
        return pl.BlockSpec(array.shape, lambda i, s: (0, 0))

    args = (*attended, w_own, *mine, *other)
    return pl.pallas_call(
        body,
        grid_spec=pltpu.PrefetchScalarGridSpec(
            num_scalar_prefetch=1,
            grid=(1,),
            in_specs=[whole(a) for a in args],
            out_specs=pl.BlockSpec((rows, 2 * span), lambda i, s: (0, 0)),
        ),
        out_shape=jax.ShapeDtypeStruct((rows, 2 * span), jnp.bfloat16),
        compiler_params=params(),
        cost_estimate=cost(16 * rows * width * span, 16 * width * span),
        name="mix",
    )(core, *args)


def local(tokens, w_query, w_key, w_value, w_out, chosen):
    tok_rows = tokens.shape[0]
    width = w_query.shape[1]
    half = tok_rows // 2
    peers = lax.axis_size(KV)
    tp = lax.axis_index("tp")
    count = lax.axis_size("tp")
    where = jnp.stack([tp, (tp + count - 1) % count, (tp + 1) % count, (tp + 2) % count]).astype(jnp.int32)
    me = jnp.reshape(lax.axis_index(KV), (1,)).astype(jnp.int32)
    core = jnp.reshape(lax.axis_index("kv_2"), (1,)).astype(jnp.int32)
    tokens, where, me, core = lax.optimization_barrier((tokens, where, me, core))

    left = shifted(tokens, "tp", 1)
    right = shifted(tokens, "tp", -1)
    request, mask = plan(me, chosen, peers)
    asked = lax.all_to_all(request, KV, 0, 0, tiled=True)

    total = project_first(where, tokens, w_key, w_value)
    top = shifted(left[:half], "tp", 1)
    bottom = shifted(right[half:], "tp", -1)
    total = project_sides(where, left, right, w_key, w_value, total)
    pair, send = project_last(where, asked, top, bottom, w_key, w_value, total)
    w_mine, send = lax.optimization_barrier((w_out, send))
    got = lax.all_to_all(send, KV, split_axis=0, concat_axis=0, tiled=True)

    span = w_out.shape[1] // 2
    part = span // 2
    piece = lax.dynamic_slice_in_dim(w_mine, core[0] * span, span, axis=1)
    w_left = shifted(piece, "tp", 1)
    w_right = shifted(piece, "tp", -1)
    w_low = shifted(w_left[:, :part], "tp", 1)
    w_high = shifted(w_right[:, part:], "tp", -1)
    mine = (w_left, w_right, w_low, w_high)
    other = tuple(shifted(w, "kv_2", 1) for w in mine)

    query = project_query(where, tokens, left, right, top, bottom, w_query)
    high, totals, summed = attend_own(query, pair, mask, peers * MOST)
    outs = attend_far(where, query, got.reshape(-1, 2 * width), mask, high, totals, summed)
    attended = (outs[0], shifted(outs[2], "tp", 1), shifted(outs[1], "tp", -1), shifted(outs[3], "tp", 2))
    return mix(core, attended, w_out, mine, other)


def solution(mesh):
    finer = Mesh(mesh.devices.reshape(4, 4, 2, mesh.shape["tp"]), ("kv_0", "kv_1", "kv_2", "tp"))
    placed = (P(KV, "tp"), P(None, "tp"), P(None, "tp"), P(None, "tp"), P("tp", None), P(KV, None))
    return jax.shard_map(
        local, mesh=finer, in_specs=placed, out_specs=P(KV_TP, None), check_vma=False
    )
```

```python
import jax
import jax.numpy as jnp
from jax import lax
from jax.experimental import pallas as pl
from jax.experimental.pallas import tpu as pltpu
from jax.sharding import Mesh
from jax.sharding import PartitionSpec as P

HD = 128
BLK = 32
MOST = 2
KV = ("kv_0", "kv_1", "kv_2")
KV_TP = ("kv_0", "kv_1", "kv_2", "tp")
NEG = -1e30
LOG2E = 1.4426950408889634
SMALL = 24 * 1024 * 1024
LARGE = 60 * 1024 * 1024
HBM = pl.BlockSpec(memory_space=pltpu.HBM)
VMEM = pl.BlockSpec(memory_space=pltpu.VMEM)
SMEM = pl.BlockSpec(memory_space=pltpu.SMEM)


def params(limit=SMALL):
    return pltpu.CompilerParams(vmem_limit_bytes=limit)


def in_hbm(shape, dtype):
    return pltpu.HBM(shape, dtype)


def in_vmem(shape, dtype):
    return pltpu.VMEM(shape, dtype)


def cost(flops, nbytes, exps=0):
    return pl.CostEstimate(flops=int(flops), bytes_accessed=int(nbytes), transcendentals=int(exps))


def keep_in_hbm(*arrays):
    return tuple(pltpu.with_memory_space_constraint(a, pltpu.HBM) for a in arrays)


def f32dot(a, b):
    return jnp.dot(a, b, preferred_element_type=jnp.float32)


def shifted(array, axis, by):
    count = lax.axis_size(axis)
    return lax.ppermute(array, axis, [(i, (i + by) % count) for i in range(count)])


def project_near(where, own, left, right, w_query, w_key, w_value):
    rows, feat = own.shape
    width = w_key.shape[1]
    chunks = where.shape[0]

    def body(where_ref, own_hbm, l_ref, r_ref, wq_hbm, wk_hbm, wv_hbm, tot_ref, qtot_hbm, wk_last, wv_last, *rest):
        own_ref, qtot, chunk_refs, sems = rest
        copies = []

        def fetch(src, dst):
            copies.append(pltpu.make_async_copy(src, dst, sems.at[len(copies)]))
            copies[-1].start()
            return copies[-1]

        first = [fetch(own_hbm, own_ref)]
        for k in range(chunks - 1):
            span = pl.ds(pl.multiple_of(where_ref[k] * feat, feat), feat)
            for j, w in enumerate((wk_hbm, wv_hbm, wq_hbm)):
                first.append(fetch(w.at[span, :], chunk_refs.at[k, j]))
        span = pl.ds(pl.multiple_of(where_ref[chunks - 1] * feat, feat), feat)
        last = [fetch(wk_hbm.at[span, :], wk_last), fetch(wv_hbm.at[span, :], wv_last)]
        first[0].wait()
        for j in range(3):
            total = None
            for k, ref in enumerate((own_ref, l_ref, r_ref)):
                first[1 + 3 * k + j].wait()
                product = f32dot(ref[...], chunk_refs[k, j])
                total = product if total is None else total + product
            if j == 2:
                qtot[...] = total
            else:
                tot_ref[:, j * width : (j + 1) * width] = total
        out = fetch(qtot, qtot_hbm)
        for copy in last:
            copy.wait()
        out.wait()

    chunk = (feat, width)
    return pl.pallas_call(
        body,
        in_specs=[SMEM, HBM, VMEM, VMEM, HBM, HBM, HBM],
        out_specs=[VMEM, HBM, VMEM, VMEM],
        out_shape=[
            in_vmem((rows, 2 * width), jnp.float32),
            in_hbm((rows, width), jnp.float32),
            in_vmem(chunk, jnp.bfloat16),
            in_vmem(chunk, jnp.bfloat16),
        ],
        scratch_shapes=[
            pltpu.VMEM((rows, feat), jnp.bfloat16),
            pltpu.VMEM((rows, width), jnp.float32),
            pltpu.VMEM((chunks - 1, 3, feat, width), jnp.bfloat16),
            pltpu.SemaphoreType.DMA((3 * chunks + 1,)),
        ],
        compiler_params=params(),
        cost_estimate=cost(18 * rows * feat * width, 30 * feat * width),
        name="project_near",
    )(where, *keep_in_hbm(own), left, right, *keep_in_hbm(w_query, w_key, w_value))


def project_last(asked, top, bottom, wk_last, wv_last, total):
    half, feat = top.shape
    rows = 2 * half
    width = wk_last.shape[1]
    peers = asked.shape[0]
    slots = peers * MOST

    def body(asked_hbm, t_ref, b_ref, wk, wv, tot_ref, pair_hbm, send_hbm, t_hbm, b_hbm, pick, pair, sem, sems, sends):
        get = pltpu.make_async_copy(asked_hbm, pick, sem)
        get.start()
        keep = [
            pltpu.make_async_copy(t_ref, t_hbm, sems.at[0]),
            pltpu.make_async_copy(b_ref, b_hbm, sems.at[1]),
        ]
        for copy in keep:
            copy.start()
        for lo, ref in ((0, t_ref), (half, b_ref)):
            span = slice(lo, lo + half)
            for j, w in enumerate((wk, wv)):
                cols = slice(j * width, (j + 1) * width)
                pair[span, cols] = (tot_ref[span, cols] + f32dot(ref[...], w[...])).astype(jnp.bfloat16)
        get.wait()
        for i in range(slots):
            block = jnp.clip(pick[i // MOST, i % MOST], 0, rows // BLK - 1)
            source = pair.at[pl.ds(pl.multiple_of(block * BLK, BLK), BLK), :]
            copy = pltpu.make_async_copy(source, send_hbm.at[i], sends.at[i])
            copy.start()
            keep.append(copy)
        copy = pltpu.make_async_copy(pair, pair_hbm, sems.at[2])
        copy.start()
        keep.append(copy)
        for copy in keep:
            copy.wait()

    return pl.pallas_call(
        body,
        in_specs=[HBM, VMEM, VMEM, VMEM, VMEM, VMEM],
        out_specs=[HBM, HBM, HBM, HBM],
        out_shape=[
            in_hbm((rows, 2 * width), jnp.bfloat16),
            in_hbm((slots, BLK, 2 * width), jnp.bfloat16),
            in_hbm((half, feat), jnp.bfloat16),
            in_hbm((half, feat), jnp.bfloat16),
        ],
        scratch_shapes=[
            pltpu.SMEM((peers, HD), jnp.int32),
            pltpu.VMEM((rows, 2 * width), jnp.bfloat16),
            pltpu.SemaphoreType.DMA,
            pltpu.SemaphoreType.DMA((3,)),
            pltpu.SemaphoreType.DMA((slots,)),
        ],
        compiler_params=params(),
        cost_estimate=cost(4 * rows * feat * width, 12 * feat * width),
        name="project_last",
    )(asked, top, bottom, wk_last, wv_last, total)


def project_query(where, top, bottom, w_query, total):
    half, feat = top.shape
    rows, width = total.shape

    def body(where_ref, t_ref, b_ref, w_ref, tot_ref, out_ref):
        for lo, ref in ((0, t_ref), (half, b_ref)):
            span = slice(lo, lo + half)
            out_ref[span, :] = (tot_ref[span, :] + f32dot(ref[...], w_ref[...])).astype(jnp.bfloat16)

    halves = pl.BlockSpec((half, feat), lambda i, s: (0, 0))
    whole = pl.BlockSpec((rows, width), lambda i, s: (0, 0))
    last = where.shape[0] - 1
    return pl.pallas_call(
        body,
        grid_spec=pltpu.PrefetchScalarGridSpec(
            num_scalar_prefetch=1,
            grid=(1,),
            in_specs=[halves, halves, pl.BlockSpec((feat, width), lambda i, s: (s[last], 0)), whole],
            out_specs=whole,
        ),
        out_shape=in_hbm((rows, width), jnp.bfloat16),
        compiler_params=params(LARGE),
        cost_estimate=cost(2 * rows * feat * width, 4 * feat * width),
        name="project_query",
    )(where, top, bottom, w_query, total)


def plan(my_index, chosen, peers):
    rows, wide = chosen.shape
    slots = peers * MOST

    def body(me_ref, cho_ref, req_ref, mask_ref):
        me = me_ref[0]
        entries = cho_ref[...]
        peer = lax.broadcasted_iota(jnp.int32, (peers, wide), 0)
        low = jnp.full((peers, wide), rows, jnp.int32)
        high = jnp.full((peers, wide), -1, jnp.int32)
        for r in range(rows):
            entry = jnp.broadcast_to(entries[r : r + 1, :], (peers, wide))
            block = entry - peer * rows
            mine = (block >= 0) & (block < rows)
            low = jnp.where(mine, jnp.minimum(low, block), low)
            high = jnp.where(mine, jnp.maximum(high, block), high)
        low = jnp.min(low, axis=1, keepdims=True)
        high = jnp.max(high, axis=1, keepdims=True)
        far = lax.broadcasted_iota(jnp.int32, (peers, 1), 0) != me
        first = jnp.where(far & (low < rows), low, -1)
        second = jnp.where(far & (high > low), high, -1)
        lane = lax.broadcasted_iota(jnp.int32, (peers, HD), 1)
        req_ref[...] = jnp.where(lane == 0, first, jnp.where(lane == 1, second, -1))
        at = lax.broadcasted_iota(jnp.int32, (peers, HD), 0)
        named = jnp.where(lane == MOST * at, first, jnp.where(lane == MOST * at + 1, second, -1))
        named = jnp.where(named >= 0, named + at * rows, -1)
        ids = jnp.max(named, axis=0, keepdims=True)
        slot = lax.broadcasted_iota(jnp.int32, (1, HD), 1)
        own = (slot >= slots) & (slot < slots + rows)
        ids = jnp.where(own, me * rows + slot - slots, ids)
        seen = entries[:, :1] == ids
        for k in range(1, wide):
            seen = seen | (entries[:, k : k + 1] == ids)
        bias = jnp.where(seen, 0.0, NEG)
        for r in range(rows):
            mask_ref[r * BLK : (r + 1) * BLK, :] = jnp.broadcast_to(bias[r : r + 1, :], (BLK, HD)).astype(jnp.bfloat16)

    return pl.pallas_call(
        body,
        grid_spec=pltpu.PrefetchScalarGridSpec(
            num_scalar_prefetch=1,
            grid=(1,),
            in_specs=[pl.BlockSpec((rows, wide), lambda i, s: (0, 0))],
            out_specs=[
                pl.BlockSpec((peers, HD), lambda i, s: (0, 0)),
                pl.BlockSpec((rows * BLK, HD), lambda i, s: (0, 0)),
            ],
        ),
        out_shape=[in_hbm((peers, HD), jnp.int32), in_hbm((rows * BLK, HD), jnp.bfloat16)],
        compiler_params=params(),
        cost_estimate=cost(1000000, 200000),
        name="plan",
    )(my_index, chosen)


def one_hot(rows, first_slot):
    slot = lax.broadcasted_iota(jnp.int32, (rows, HD), 0) // BLK + first_slot
    return (slot == lax.broadcasted_iota(jnp.int32, (rows, HD), 1)).astype(jnp.bfloat16)


def scores_of(query, keys):
    return lax.dot_general(query, keys, (((1,), (1,)), ((), ())), preferred_element_type=jnp.float32)


def attend_own(query, pair, mask, first_slot):
    rows, width = query.shape
    heads = width // HD
    scale = HD ** (-0.5) * LOG2E
    tile = 256

    def body(q_ref, k_ref, v_ref, mask_ref, high_ref, tot_ref, sum_ref):
        keys = jnp.concatenate([k_ref[...], one_hot(rows, first_slot)], axis=1)
        values = jnp.concatenate([v_ref[...], jnp.ones_like(v_ref)], axis=1)
        for lo in range(0, rows, tile):
            span = slice(lo, lo + tile)
            count = lo + tile
            wide = jnp.concatenate([q_ref[span, :], mask_ref[span, :]], axis=1)
            scores = scores_of(wide, keys[:count])
            row = lax.broadcasted_iota(jnp.int32, scores.shape, 0) + lo
            col = lax.broadcasted_iota(jnp.int32, scores.shape, 1)
            scores = jnp.where(col <= row, scores, NEG)
            high = jnp.max(scores, axis=1, keepdims=True)
            weights = jnp.exp2((scores - high) * scale).astype(jnp.bfloat16)
            summed = f32dot(weights, values[:count])
            high_ref[span, :] = jnp.broadcast_to(high, (tile, HD))
            tot_ref[span, :] = summed[:, HD:]
            sum_ref[span, :] = summed[:, :HD]

    column = pl.BlockSpec((rows, HD), lambda h: (0, h))
    return pl.pallas_call(
        body,
        grid=(heads,),
        in_specs=[
            column,
            column,
            pl.BlockSpec((rows, HD), lambda h: (0, heads + h)),
            pl.BlockSpec((rows, HD), lambda h: (0, 0)),
        ],
        out_specs=[column, column, column],
        out_shape=[in_hbm((rows, width), jnp.float32)] * 3,
        compiler_params=params(LARGE),
        cost_estimate=cost(8 * rows * rows * width, 16 * rows * width, rows * rows * heads),
        name="attend_own",
    )(query, pair, pair, mask)


def attend_far(where, query, got, mask, high, total, summed):
    rows, width = query.shape
    heads = width // HD
    count = got.shape[0]
    scale = HD ** (-0.5) * LOG2E
    parts = where.shape[0]
    tile = rows // parts
    pairs = ((3, 1), (2, 0))

    def body(where_ref, q_ref, k_ref, v_ref, mask_ref, high_ref, tot_ref, sum_ref, *rest):
        outs, keys, values = rest[:parts], rest[parts], rest[parts + 1]

        @pl.when(pl.program_id(0) == 0)
        def _():
            keys[:, HD:] = one_hot(count, 0)
            values[:, HD:] = jnp.ones_like(v_ref)

        keys[:, :HD] = k_ref[...]
        values[:, :HD] = v_ref[...]

        def rows_of(ref, parts_at):
            spans = [pl.ds(pl.multiple_of(where_ref[p] * tile, tile), tile) for p in parts_at]
            return jnp.concatenate([ref[span, :] for span in spans], axis=0)

        def scores_at(parts_at):
            wide = jnp.concatenate([rows_of(q_ref, parts_at), rows_of(mask_ref, parts_at)], axis=1)
            return scores_of(wide, keys[...])

        later = scores_at(pairs[0])
        for i, parts_at in enumerate(pairs):
            scores = later
            if i + 1 < len(pairs):
                later = scores_at(pairs[i + 1])
            own = rows_of(high_ref, parts_at)
            top = jnp.maximum(jnp.max(scores, axis=1, keepdims=True), own[:, :1])
            weights = jnp.exp2((scores - top) * scale).astype(jnp.bfloat16)
            far = f32dot(weights, values[...])
            keep = jnp.exp2((own - top) * scale)
            result = far[:, :HD] + keep * rows_of(sum_ref, parts_at)
            result = (result / (far[:, HD:] + keep * rows_of(tot_ref, parts_at))).astype(jnp.bfloat16)
            for k, part in enumerate(parts_at):
                outs[part][...] = result[k * tile : (k + 1) * tile]

    column = pl.BlockSpec((rows, HD), lambda h, s: (0, h))
    return pl.pallas_call(
        body,
        grid_spec=pltpu.PrefetchScalarGridSpec(
            num_scalar_prefetch=1,
            grid=(heads,),
            in_specs=[
                column,
                pl.BlockSpec((count, HD), lambda h, s: (0, h)),
                pl.BlockSpec((count, HD), lambda h, s: (0, heads + h)),
                pl.BlockSpec((rows, HD), lambda h, s: (0, 0)),
                column,
                column,
                column,
            ],
            out_specs=[pl.BlockSpec((tile, HD), lambda h, s: (0, h))] * parts,
            scratch_shapes=[pltpu.VMEM((count, 2 * HD), jnp.bfloat16)] * 2,
        ),
        out_shape=[jax.ShapeDtypeStruct((tile, width), jnp.bfloat16)] * parts,
        compiler_params=params(),
        cost_estimate=cost(8 * rows * count * width, 4 * count * width, rows * count * heads),
        name="attend_far",
    )(where, *keep_in_hbm(query, got, got, mask, high, total, summed))


def mix(core, attended, w_own, mine, other):
    rows, width = attended[0].shape
    span = mine[0].shape[1]
    part = mine[2].shape[1]

    def body(core_ref, own_ref, l_ref, r_ref, f_ref, w_ref, *rest):
        out_ref = rest[-1]
        for which, pieces in ((core_ref[0], rest[:4]), (1 - core_ref[0], rest[4:8])):
            at = pl.multiple_of(which * span, span)
            total = f32dot(own_ref[...], w_ref[:, pl.ds(at, span)])
            total = total + f32dot(l_ref[...], pieces[0][...]) + f32dot(r_ref[...], pieces[1][...])
            low = total[:, :part] + f32dot(f_ref[...], pieces[2][...])
            high = total[:, part:] + f32dot(f_ref[...], pieces[3][...])
            out_ref[:, pl.ds(at, part)] = low.astype(jnp.bfloat16)
            out_ref[:, pl.ds(at + part, part)] = high.astype(jnp.bfloat16)

    def whole(array):
        return pl.BlockSpec(array.shape, lambda i, s: (0, 0))

    args = (*attended, w_own, *mine, *other)
    return pl.pallas_call(
        body,
        grid_spec=pltpu.PrefetchScalarGridSpec(
            num_scalar_prefetch=1,
            grid=(1,),
            in_specs=[whole(a) for a in args],
            out_specs=pl.BlockSpec((rows, 2 * span), lambda i, s: (0, 0)),
        ),
        out_shape=jax.ShapeDtypeStruct((rows, 2 * span), jnp.bfloat16),
        compiler_params=params(),
        cost_estimate=cost(16 * rows * width * span, 16 * width * span),
        name="mix",
    )(core, *args)


def local(tokens, w_query, w_key, w_value, w_out, chosen):
    tok_rows = tokens.shape[0]
    width = w_query.shape[1]
    half = tok_rows // 2
    peers = lax.axis_size(KV)
    tp = lax.axis_index("tp")
    count = lax.axis_size("tp")
    where = jnp.stack([tp, (tp + count - 1) % count, (tp + 1) % count, (tp + 2) % count]).astype(jnp.int32)
    me = jnp.reshape(lax.axis_index(KV), (1,)).astype(jnp.int32)
    core = jnp.reshape(lax.axis_index("kv_2"), (1,)).astype(jnp.int32)
    tokens, where, me, core = lax.optimization_barrier((tokens, where, me, core))

    left = shifted(tokens, "tp", 1)
    right = shifted(tokens, "tp", -1)
    request, mask = plan(me, chosen, peers)
    asked = lax.all_to_all(request, KV, 0, 0, tiled=True)
    left, right, asked, mask = lax.optimization_barrier((left, right, asked, mask))

    top = shifted(left[:half], "tp", 1)
    bottom = shifted(right[half:], "tp", -1)
    total, q_total, wk_last, wv_last = project_near(where, tokens, left, right, w_query, w_key, w_value)
    pair, send, top, bottom = project_last(asked, top, bottom, wk_last, wv_last, total)
    w_mine, send = lax.optimization_barrier((w_out, send))
    got = lax.all_to_all(send, KV, split_axis=0, concat_axis=0, tiled=True)

    span = w_out.shape[1] // 2
    part = span // 2
    piece = lax.dynamic_slice_in_dim(w_mine, core[0] * span, span, axis=1)
    w_left = shifted(piece, "tp", 1)
    w_right = shifted(piece, "tp", -1)
    w_low = shifted(w_left[:, :part], "tp", 1)
    w_high = shifted(w_right[:, part:], "tp", -1)
    mine = (w_left, w_right, w_low, w_high)
    other = tuple(shifted(w, "kv_2", 1) for w in mine)

    query = project_query(where, top, bottom, w_query, q_total)
    high, totals, summed = attend_own(query, pair, mask, peers * MOST)
    outs = attend_far(where, query, got.reshape(-1, 2 * width), mask, high, totals, summed)
    attended = (outs[0], shifted(outs[2], "tp", 1), shifted(outs[1], "tp", -1), shifted(outs[3], "tp", 2))
    return mix(core, attended, w_out, mine, other)


def solution(mesh):
    finer = Mesh(mesh.devices.reshape(4, 4, 2, mesh.shape["tp"]), ("kv_0", "kv_1", "kv_2", "tp"))
    placed = (P(KV, "tp"), P(None, "tp"), P(None, "tp"), P(None, "tp"), P("tp", None), P(KV, None))
    return jax.shard_map(
        local, mesh=finer, in_specs=placed, out_specs=P(KV_TP, None), check_vma=False
    )
```

```python
import jax
import jax.numpy as jnp
from jax import lax
from jax.experimental import pallas as pl
from jax.experimental.pallas import tpu as pltpu
from jax.sharding import Mesh
from jax.sharding import PartitionSpec as P


HD = 128
BLK = 32
MOST = 2
KV = ("kv_0", "kv_1", "kv_2")
KV_TP = ("kv_0", "kv_1", "kv_2", "tp")
NEG = -1e30
LOG2E = 1.4426950408889634
SMALL = 24 * 1024 * 1024
LARGE = 60 * 1024 * 1024
HBM = pl.BlockSpec(memory_space=pltpu.HBM)
VMEM = pl.BlockSpec(memory_space=pltpu.VMEM)
SMEM = pl.BlockSpec(memory_space=pltpu.SMEM)


def params(limit=SMALL):
    return pltpu.CompilerParams(vmem_limit_bytes=limit)


def in_hbm(shape, dtype):
    return pltpu.HBM(shape, dtype)


def in_vmem(shape, dtype):
    return pltpu.VMEM(shape, dtype)


def cost(flops, nbytes, exps=0):
    return pl.CostEstimate(flops=int(flops), bytes_accessed=int(nbytes), transcendentals=int(exps))


def keep_in_hbm(*arrays):
    return tuple(pltpu.with_memory_space_constraint(a, pltpu.HBM) for a in arrays)


def f32dot(a, b):
    return jnp.dot(a, b, preferred_element_type=jnp.float32)


def shifted(array, axis, by):
    count = lax.axis_size(axis)
    return lax.ppermute(array, axis, [(i, (i + by) % count) for i in range(count)])


def project_near(where, own, left, right, w_key, w_value):
    rows, feat = own.shape
    width = w_key.shape[1]
    chunks = where.shape[0]

    def body(where_ref, own_hbm, l_ref, r_ref, wk_hbm, wv_hbm, tot_ref, wk_last, wv_last, l_hbm, r_hbm, *rest):
        own_ref, chunk_refs, sems = rest
        copies = []

        def fetch(src, dst):
            copies.append(pltpu.make_async_copy(src, dst, sems.at[len(copies)]))
            copies[-1].start()
            return copies[-1]

        own_copy = fetch(own_hbm, own_ref)
        pieces = []
        for k in range(chunks - 1):
            span = pl.ds(pl.multiple_of(where_ref[k] * feat, feat), feat)
            for j, w in enumerate((wk_hbm, wv_hbm)):
                pieces.append(fetch(w.at[span, :], chunk_refs.at[k, j]))
        span = pl.ds(pl.multiple_of(where_ref[chunks - 1] * feat, feat), feat)
        last = [fetch(wk_hbm.at[span, :], wk_last), fetch(wv_hbm.at[span, :], wv_last)]
        last += [fetch(l_ref, l_hbm), fetch(r_ref, r_hbm)]
        own_copy.wait()
        for copy in pieces:
            copy.wait()
        for j in range(2):
            total = f32dot(own_ref[...], chunk_refs[0, j]) + f32dot(l_ref[...], chunk_refs[1, j])
            tot_ref[:, j * width : (j + 1) * width] = total + f32dot(r_ref[...], chunk_refs[2, j])
        for copy in last:
            copy.wait()

    chunk = (feat, width)
    return pl.pallas_call(
        body,
        in_specs=[SMEM, HBM, VMEM, VMEM, HBM, HBM],
        out_specs=[VMEM, VMEM, VMEM, HBM, HBM],
        out_shape=[
            in_vmem((rows, 2 * width), jnp.float32),
            in_vmem(chunk, jnp.bfloat16),
            in_vmem(chunk, jnp.bfloat16),
            in_hbm((rows, feat), jnp.bfloat16),
            in_hbm((rows, feat), jnp.bfloat16),
        ],
        scratch_shapes=[
            pltpu.VMEM((rows, feat), jnp.bfloat16),
            pltpu.VMEM((chunks - 1, 2, feat, width), jnp.bfloat16),
            pltpu.SemaphoreType.DMA((2 * chunks + 3,)),
        ],
        compiler_params=params(),
        cost_estimate=cost(12 * rows * feat * width, 20 * feat * width),
        name="project_near",
    )(where, *keep_in_hbm(own), left, right, *keep_in_hbm(w_key, w_value))


def project_last(asked, top, bottom, wk_last, wv_last, total):
    half, feat = top.shape
    rows = 2 * half
    width = wk_last.shape[1]
    peers = asked.shape[0]
    slots = peers * MOST

    def body(asked_hbm, t_ref, b_ref, wk, wv, tot_ref, pair_hbm, send_hbm, t_hbm, b_hbm, pick, pair, sem, sems, sends):
        get = pltpu.make_async_copy(asked_hbm, pick, sem)
        get.start()
        keep = [
            pltpu.make_async_copy(t_ref, t_hbm, sems.at[0]),
            pltpu.make_async_copy(b_ref, b_hbm, sems.at[1]),
        ]
        for copy in keep:
            copy.start()
        for lo, ref in ((0, t_ref), (half, b_ref)):
            span = slice(lo, lo + half)
            for j, w in enumerate((wk, wv)):
                cols = slice(j * width, (j + 1) * width)
                pair[span, cols] = (tot_ref[span, cols] + f32dot(ref[...], w[...])).astype(jnp.bfloat16)
        get.wait()
        for i in range(slots):
            block = jnp.clip(pick[i // MOST, i % MOST], 0, rows // BLK - 1)
            source = pair.at[pl.ds(pl.multiple_of(block * BLK, BLK), BLK), :]
            copy = pltpu.make_async_copy(source, send_hbm.at[i], sends.at[i])
            copy.start()
            keep.append(copy)
        copy = pltpu.make_async_copy(pair, pair_hbm, sems.at[2])
        copy.start()
        keep.append(copy)
        for copy in keep:
            copy.wait()

    return pl.pallas_call(
        body,
        in_specs=[HBM, VMEM, VMEM, VMEM, VMEM, VMEM],
        out_specs=[HBM, HBM, HBM, HBM],
        out_shape=[
            in_hbm((rows, 2 * width), jnp.bfloat16),
            in_hbm((slots, BLK, 2 * width), jnp.bfloat16),
            in_hbm((half, feat), jnp.bfloat16),
            in_hbm((half, feat), jnp.bfloat16),
        ],
        scratch_shapes=[
            pltpu.SMEM((peers, HD), jnp.int32),
            pltpu.VMEM((rows, 2 * width), jnp.bfloat16),
            pltpu.SemaphoreType.DMA,
            pltpu.SemaphoreType.DMA((3,)),
            pltpu.SemaphoreType.DMA((slots,)),
        ],
        compiler_params=params(),
        cost_estimate=cost(4 * rows * feat * width, 12 * feat * width),
        name="project_last",
    )(asked, top, bottom, wk_last, wv_last, total)


def project_query(where, own, left, right, top, bottom, w_query):
    rows, feat = own.shape
    half = top.shape[0]
    width = w_query.shape[1]

    def body(where_ref, o_ref, l_ref, r_ref, t_ref, b_ref, wo, wl, wr, wf, out_ref):
        for lo, far in ((0, t_ref), (half, b_ref)):
            span = slice(lo, lo + half)
            total = f32dot(o_ref[span, :], wo[...]) + f32dot(l_ref[span, :], wl[...])
            total = total + f32dot(r_ref[span, :], wr[...]) + f32dot(far[...], wf[...])
            out_ref[span, :] = total.astype(jnp.bfloat16)

    def chunk(k):
        return pl.BlockSpec((feat, width), lambda i, s: (s[k], 0))

    toks = pl.BlockSpec((rows, feat), lambda i, s: (0, 0))
    halves = pl.BlockSpec((half, feat), lambda i, s: (0, 0))
    return pl.pallas_call(
        body,
        grid_spec=pltpu.PrefetchScalarGridSpec(
            num_scalar_prefetch=1,
            grid=(1,),
            in_specs=[toks, toks, toks, halves, halves, chunk(0), chunk(1), chunk(2), chunk(3)],
            out_specs=pl.BlockSpec((rows, width), lambda i, s: (0, 0)),
        ),
        out_shape=in_hbm((rows, width), jnp.bfloat16),
        compiler_params=params(LARGE),
        cost_estimate=cost(8 * rows * feat * width, 16 * feat * width),
        name="project_query",
    )(where, *keep_in_hbm(own, left, right, top, bottom, w_query, w_query, w_query, w_query))


def plan(my_index, chosen, peers):
    rows, wide = chosen.shape
    slots = peers * MOST

    def body(me_ref, cho_ref, req_ref, mask_ref):
        me = me_ref[0]
        entries = cho_ref[...]
        peer = lax.broadcasted_iota(jnp.int32, (peers, wide), 0)
        low = jnp.full((peers, wide), rows, jnp.int32)
        high = jnp.full((peers, wide), -1, jnp.int32)
        for r in range(rows):
            entry = jnp.broadcast_to(entries[r : r + 1, :], (peers, wide))
            block = entry - peer * rows
            mine = (block >= 0) & (block < rows)
            low = jnp.where(mine, jnp.minimum(low, block), low)
            high = jnp.where(mine, jnp.maximum(high, block), high)
        low = jnp.min(low, axis=1, keepdims=True)
        high = jnp.max(high, axis=1, keepdims=True)
        far = lax.broadcasted_iota(jnp.int32, (peers, 1), 0) != me
        first = jnp.where(far & (low < rows), low, -1)
        second = jnp.where(far & (high > low), high, -1)
        lane = lax.broadcasted_iota(jnp.int32, (peers, HD), 1)
        req_ref[...] = jnp.where(lane == 0, first, jnp.where(lane == 1, second, -1))
        at = lax.broadcasted_iota(jnp.int32, (peers, HD), 0)
        named = jnp.where(lane == MOST * at, first, jnp.where(lane == MOST * at + 1, second, -1))
        named = jnp.where(named >= 0, named + at * rows, -1)
        ids = jnp.max(named, axis=0, keepdims=True)
        slot = lax.broadcasted_iota(jnp.int32, (1, HD), 1)
        own = (slot >= slots) & (slot < slots + rows)
        ids = jnp.where(own, me * rows + slot - slots, ids)
        seen = entries[:, :1] == ids
        for k in range(1, wide):
            seen = seen | (entries[:, k : k + 1] == ids)
        bias = jnp.where(seen, 0.0, NEG)
        for r in range(rows):
            mask_ref[r * BLK : (r + 1) * BLK, :] = jnp.broadcast_to(bias[r : r + 1, :], (BLK, HD)).astype(jnp.bfloat16)

    return pl.pallas_call(
        body,
        grid_spec=pltpu.PrefetchScalarGridSpec(
            num_scalar_prefetch=1,
            grid=(1,),
            in_specs=[pl.BlockSpec((rows, wide), lambda i, s: (0, 0))],
            out_specs=[
                pl.BlockSpec((peers, HD), lambda i, s: (0, 0)),
                pl.BlockSpec((rows * BLK, HD), lambda i, s: (0, 0)),
            ],
        ),
        out_shape=[in_hbm((peers, HD), jnp.int32), in_hbm((rows * BLK, HD), jnp.bfloat16)],
        compiler_params=params(),
        cost_estimate=cost(1000000, 200000),
        name="plan",
    )(my_index, chosen)


def one_hot(rows, first_slot):
    slot = lax.broadcasted_iota(jnp.int32, (rows, HD), 0) // BLK + first_slot
    return (slot == lax.broadcasted_iota(jnp.int32, (rows, HD), 1)).astype(jnp.bfloat16)


def scores_of(query, keys):
    return lax.dot_general(query, keys, (((1,), (1,)), ((), ())), preferred_element_type=jnp.float32)


def attend_own(query, pair, mask, first_slot):
    rows, width = query.shape
    heads = width // HD
    scale = HD ** (-0.5) * LOG2E
    tile = 256

    def body(q_ref, k_ref, v_ref, mask_ref, high_ref, tot_ref, sum_ref):
        keys = jnp.concatenate([k_ref[...], one_hot(rows, first_slot)], axis=1)
        values = jnp.concatenate([v_ref[...], jnp.ones_like(v_ref)], axis=1)
        for lo in range(0, rows, tile):
            span = slice(lo, lo + tile)
            count = lo + tile
            wide = jnp.concatenate([q_ref[span, :], mask_ref[span, :]], axis=1)
            scores = scores_of(wide, keys[:count])
            row = lax.broadcasted_iota(jnp.int32, scores.shape, 0) + lo
            col = lax.broadcasted_iota(jnp.int32, scores.shape, 1)
            scores = jnp.where(col <= row, scores, NEG)
            high = jnp.max(scores, axis=1, keepdims=True)
            weights = jnp.exp2((scores - high) * scale).astype(jnp.bfloat16)
            summed = f32dot(weights, values[:count])
            high_ref[span, :] = jnp.broadcast_to(high, (tile, HD))
            tot_ref[span, :] = summed[:, HD:]
            sum_ref[span, :] = summed[:, :HD]

    column = pl.BlockSpec((rows, HD), lambda h: (0, h))
    return pl.pallas_call(
        body,
        grid=(heads,),
        in_specs=[
            column,
            column,
            pl.BlockSpec((rows, HD), lambda h: (0, heads + h)),
            pl.BlockSpec((rows, HD), lambda h: (0, 0)),
        ],
        out_specs=[column, column, column],
        out_shape=[in_hbm((rows, width), jnp.float32)] * 3,
        compiler_params=params(LARGE),
        cost_estimate=cost(8 * rows * rows * width, 16 * rows * width, rows * rows * heads),
        name="attend_own",
    )(query, pair, pair, mask)


def far_rows(where_ref, parts, tile):
    def rows_of(ref, cols=slice(None)):
        spans = [pl.ds(pl.multiple_of(where_ref[p] * tile, tile), tile) for p in parts]
        return jnp.concatenate([ref[span, cols] for span in spans], axis=0)

    return rows_of


def finished(scores, values, high, total, summed):
    scale = HD ** (-0.5) * LOG2E
    top = jnp.maximum(jnp.max(scores, axis=1, keepdims=True), high[:, :1])
    weights = jnp.exp2((scores - top) * scale).astype(jnp.bfloat16)
    far = f32dot(weights, values)
    keep = jnp.exp2((high - top) * scale)
    return ((far[:, :HD] + keep * summed) / (far[:, HD:] + keep * total)).astype(jnp.bfloat16)


def attend_far(where, query, got, mask, high, total, summed, parts):
    rows, width = query.shape
    heads = width // HD
    count = got.shape[0]
    tile = rows // where.shape[0]

    def body(where_ref, q_ref, k_ref, v_ref, mask_ref, high_ref, tot_ref, sum_ref, out_a, out_b, keys_out, values_out):
        rows_of = far_rows(where_ref, parts, tile)
        keys, values = keys_out.at[pl.program_id(0)], values_out.at[pl.program_id(0)]
        keys[:, HD:] = one_hot(count, 0)
        keys[:, :HD] = k_ref[...]
        wide = jnp.concatenate([rows_of(q_ref), rows_of(mask_ref)], axis=1)
        scores = scores_of(wide, keys[...])
        values[:, HD:] = jnp.ones_like(v_ref)
        values[:, :HD] = v_ref[...]
        result = finished(scores, values[...], rows_of(high_ref), rows_of(tot_ref), rows_of(sum_ref))
        out_a[...] = result[:tile]
        out_b[...] = result[tile:]

    column = pl.BlockSpec((rows, HD), lambda h, s: (0, h))
    wides = in_vmem((heads, count, 2 * HD), jnp.bfloat16)
    return pl.pallas_call(
        body,
        grid_spec=pltpu.PrefetchScalarGridSpec(
            num_scalar_prefetch=1,
            grid=(heads,),
            in_specs=[
                column,
                pl.BlockSpec((count, HD), lambda h, s: (0, h)),
                pl.BlockSpec((count, HD), lambda h, s: (0, heads + h)),
                pl.BlockSpec((rows, HD), lambda h, s: (0, 0)),
                column,
                column,
                column,
            ],
            out_specs=[pl.BlockSpec((tile, HD), lambda h, s: (0, h))] * 2 + [VMEM] * 2,
        ),
        out_shape=[jax.ShapeDtypeStruct((tile, width), jnp.bfloat16)] * 2 + [wides] * 2,
        compiler_params=params(),
        cost_estimate=cost(4 * rows * count * width, 4 * count * width, rows * count * heads),
        name="attend_far",
    )(where, *keep_in_hbm(query, got, got, mask, high, total, summed))


def attend_rest(where, query, keys, values, mask, high, total, summed, parts):
    rows, width = query.shape
    heads, count, _ = keys.shape
    tile = rows // where.shape[0]

    def body(where_ref, q_ref, keys_ref, values_ref, mask_ref, high_ref, tot_ref, sum_ref, out_a, out_b):
        rows_of = far_rows(where_ref, parts, tile)

        def scores_at(h):
            query = rows_of(q_ref, slice(h * HD, (h + 1) * HD))
            return scores_of(jnp.concatenate([query, rows_of(mask_ref)], axis=1), keys_ref[h])

        later = scores_at(0)
        for h in range(heads):
            scores = later
            if h + 1 < heads:
                later = scores_at(h + 1)
            cols = slice(h * HD, (h + 1) * HD)
            own = [rows_of(ref, cols) for ref in (high_ref, tot_ref, sum_ref)]
            result = finished(scores, values_ref[h], *own)
            out_a[:, cols] = result[:tile]
            out_b[:, cols] = result[tile:]

    def whole(array):
        return pl.BlockSpec(array.shape, lambda i, s: (0, 0))

    return pl.pallas_call(
        body,
        grid_spec=pltpu.PrefetchScalarGridSpec(
            num_scalar_prefetch=1,
            grid=(1,),
            in_specs=[whole(query), VMEM, VMEM, whole(mask), whole(high), whole(total), whole(summed)],
            out_specs=[pl.BlockSpec((tile, width), lambda i, s: (0, 0))] * 2,
        ),
        out_shape=[jax.ShapeDtypeStruct((tile, width), jnp.bfloat16)] * 2,
        compiler_params=params(),
        cost_estimate=cost(4 * rows * count * width, 4 * count * width, rows * count * heads),
        name="attend_rest",
    )(where, *keep_in_hbm(query), keys, values, *keep_in_hbm(mask, high, total, summed))


def mix_near(core, own, right, far, w_own, w_right, w_far):
    rows = own.shape[0]
    span = w_right[0].shape[1]
    part = w_far[0].shape[1]

    def body(core_ref, own_ref, r_ref, f_ref, w_ref, *rest):
        out_ref = rest[-1]
        for side, which in enumerate((core_ref[0], 1 - core_ref[0])):
            at = pl.multiple_of(which * span, span)
            total = f32dot(own_ref[...], w_ref[:, pl.ds(at, span)]) + f32dot(r_ref[...], rest[side][...])
            for k in range(2):
                far_part = f32dot(f_ref[...], rest[2 + 2 * side + k][...])
                out_ref[:, pl.ds(at + k * part, part)] = total[:, k * part : (k + 1) * part] + far_part

    args = (own, right, far, w_own, *w_right, *w_far)
    return pl.pallas_call(
        body,
        in_specs=[SMEM] + [VMEM] * len(args),
        out_specs=VMEM,
        out_shape=in_vmem((rows, 2 * span), jnp.float32),
        compiler_params=params(),
        cost_estimate=cost(12 * rows * own.shape[1] * span, 12 * own.shape[1] * span),
        name="mix_near",
    )(core, *args)


def mix_last(core, left, w_left, before):
    rows = left.shape[0]
    span = w_left[0].shape[1]

    def body(core_ref, l_ref, mine_ref, other_ref, before_ref, out_ref):
        for which, ref in ((core_ref[0], mine_ref), (1 - core_ref[0], other_ref)):
            to = pl.ds(pl.multiple_of(which * span, span), span)
            out_ref[:, to] = (before_ref[:, to] + f32dot(l_ref[...], ref[...])).astype(jnp.bfloat16)

    return pl.pallas_call(
        body,
        in_specs=[SMEM] + [VMEM] * 4,
        out_specs=VMEM,
        out_shape=jax.ShapeDtypeStruct((rows, 2 * span), jnp.bfloat16),
        compiler_params=params(),
        cost_estimate=cost(4 * rows * left.shape[1] * span, 4 * left.shape[1] * span),
        name="mix_last",
    )(core, left, *w_left, before)


def local(tokens, w_query, w_key, w_value, w_out, chosen):
    tok_rows = tokens.shape[0]
    width = w_query.shape[1]
    half = tok_rows // 2
    peers = lax.axis_size(KV)
    tp = lax.axis_index("tp")
    count = lax.axis_size("tp")
    where = jnp.stack([tp, (tp + count - 1) % count, (tp + 1) % count, (tp + 2) % count]).astype(jnp.int32)
    me = jnp.reshape(lax.axis_index(KV), (1,)).astype(jnp.int32)
    core = jnp.reshape(lax.axis_index("kv_2"), (1,)).astype(jnp.int32)
    tokens, where, me, core = lax.optimization_barrier((tokens, where, me, core))

    left = shifted(tokens, "tp", 1)
    right = shifted(tokens, "tp", -1)
    request, mask = plan(me, chosen, peers)
    asked = lax.all_to_all(request, KV, 0, 0, tiled=True)
    left, right, request, mask = lax.optimization_barrier((left, right, request, mask))

    top = shifted(left[:half], "tp", 1)
    bottom = shifted(right[half:], "tp", -1)
    total, wk_last, wv_last, left, right = project_near(where, tokens, left, right, w_key, w_value)
    pair, send, top, bottom = project_last(asked, top, bottom, wk_last, wv_last, total)
    w_mine, send = lax.optimization_barrier((w_out, send))
    got = lax.all_to_all(send, KV, split_axis=0, concat_axis=0, tiled=True)

    span = w_out.shape[1] // 2
    part = span // 2
    piece = lax.dynamic_slice_in_dim(w_mine, core[0] * span, span, axis=1)
    w_left = shifted(piece, "tp", 1)
    w_right = shifted(piece, "tp", -1)
    w_low = shifted(w_left[:, :part], "tp", 1)
    w_high = shifted(w_right[:, part:], "tp", -1)
    w_left = (w_left, shifted(w_left, "kv_2", 1))
    w_right = (w_right, shifted(w_right, "kv_2", 1))
    w_far = (w_low, w_high, shifted(w_low, "kv_2", 1), shifted(w_high, "kv_2", 1))

    query = project_query(where, tokens, left, right, top, bottom, w_query)
    high, totals, summed = attend_own(query, pair, mask, peers * MOST)
    got = got.reshape(-1, 2 * width)
    to_far, to_left, keys, values = attend_far(where, query, got, mask, high, totals, summed, (3, 1))
    far = shifted(to_far, "tp", 2)
    right = shifted(to_left, "tp", -1)
    to_right, own = attend_rest(where, query, keys, values, mask, high, totals, summed, (2, 0))
    left = shifted(to_right, "tp", 1)
    before = mix_near(core, own, right, far, w_out, w_right, w_far)
    return mix_last(core, left, w_left, before)


def solution(mesh):
    finer = Mesh(mesh.devices.reshape(4, 4, 2, mesh.shape["tp"]), ("kv_0", "kv_1", "kv_2", "tp"))
    placed = (P(KV, "tp"), P(None, "tp"), P(None, "tp"), P(None, "tp"), P("tp", None), P(KV, None))

    return jax.shard_map(local, mesh=finer, in_specs=placed, out_specs=P(KV_TP, None), check_vma=False)
```

```python
import jax
import jax.numpy as jnp
from jax import lax
from jax.experimental import pallas as pl
from jax.experimental.pallas import tpu as pltpu
from jax.sharding import Mesh
from jax.sharding import PartitionSpec as P


HD = 128
BLK = 32
MOST = 2
KV = ("kv_0", "kv_1", "kv_2")
KV_TP = ("kv_0", "kv_1", "kv_2", "tp")
NEG = -1e30
LOG2E = 1.4426950408889634
SMALL = 24 * 1024 * 1024
LARGE = 60 * 1024 * 1024
HBM = pl.BlockSpec(memory_space=pltpu.HBM)
VMEM = pl.BlockSpec(memory_space=pltpu.VMEM)
SMEM = pl.BlockSpec(memory_space=pltpu.SMEM)


def params(limit=SMALL):
    return pltpu.CompilerParams(vmem_limit_bytes=limit)


def in_hbm(shape, dtype):
    return pltpu.HBM(shape, dtype)


def in_vmem(shape, dtype):
    return pltpu.VMEM(shape, dtype)


def cost(flops, nbytes, exps=0):
    return pl.CostEstimate(flops=int(flops), bytes_accessed=int(nbytes), transcendentals=int(exps))


def keep_in_hbm(*arrays):
    return tuple(pltpu.with_memory_space_constraint(a, pltpu.HBM) for a in arrays)


def f32dot(a, b):
    return jnp.dot(a, b, preferred_element_type=jnp.float32)


def shifted(array, axis, by):
    count = lax.axis_size(axis)
    return lax.ppermute(array, axis, [(i, (i + by) % count) for i in range(count)])


def project_near(where, own, left, right, w_key, w_value):
    rows, feat = own.shape
    width = w_key.shape[1]
    chunks = where.shape[0]

    def body(where_ref, own_hbm, l_ref, r_ref, wk_hbm, wv_hbm, tot_ref, wk_last, wv_last, l_hbm, r_hbm, *rest):
        own_ref, chunk_refs, sems = rest
        copies = []

        def fetch(src, dst):
            copies.append(pltpu.make_async_copy(src, dst, sems.at[len(copies)]))
            copies[-1].start()
            return copies[-1]

        own_copy = fetch(own_hbm, own_ref)
        pieces = []
        for k in range(chunks - 1):
            span = pl.ds(pl.multiple_of(where_ref[k] * feat, feat), feat)
            for j, w in enumerate((wk_hbm, wv_hbm)):
                pieces.append(fetch(w.at[span, :], chunk_refs.at[k, j]))
        span = pl.ds(pl.multiple_of(where_ref[chunks - 1] * feat, feat), feat)
        last = [fetch(wk_hbm.at[span, :], wk_last), fetch(wv_hbm.at[span, :], wv_last)]
        last += [fetch(l_ref, l_hbm), fetch(r_ref, r_hbm)]
        own_copy.wait()
        for copy in pieces:
            copy.wait()
        for j in range(2):
            total = f32dot(own_ref[...], chunk_refs[0, j]) + f32dot(l_ref[...], chunk_refs[1, j])
            tot_ref[:, j * width : (j + 1) * width] = total + f32dot(r_ref[...], chunk_refs[2, j])
        for copy in last:
            copy.wait()

    chunk = (feat, width)
    return pl.pallas_call(
        body,
        in_specs=[SMEM, HBM, VMEM, VMEM, HBM, HBM],
        out_specs=[VMEM, VMEM, VMEM, HBM, HBM],
        out_shape=[
            in_vmem((rows, 2 * width), jnp.float32),
            in_vmem(chunk, jnp.bfloat16),
            in_vmem(chunk, jnp.bfloat16),
            in_hbm((rows, feat), jnp.bfloat16),
            in_hbm((rows, feat), jnp.bfloat16),
        ],
        scratch_shapes=[
            pltpu.VMEM((rows, feat), jnp.bfloat16),
            pltpu.VMEM((chunks - 1, 2, feat, width), jnp.bfloat16),
            pltpu.SemaphoreType.DMA((2 * chunks + 3,)),
        ],
        compiler_params=params(),
        cost_estimate=cost(12 * rows * feat * width, 20 * feat * width),
        name="project_near",
    )(where, *keep_in_hbm(own), left, right, *keep_in_hbm(w_key, w_value))


def project_last(asked, top, bottom, wk_last, wv_last, total):
    half, feat = top.shape
    rows = 2 * half
    width = wk_last.shape[1]
    peers = asked.shape[0]
    slots = peers * MOST

    def body(asked_hbm, t_ref, b_ref, wk, wv, tot_ref, pair_hbm, send_hbm, t_hbm, b_hbm, pick, pair, sem, sems, sends):
        get = pltpu.make_async_copy(asked_hbm, pick, sem)
        get.start()
        keep = [
            pltpu.make_async_copy(t_ref, t_hbm, sems.at[0]),
            pltpu.make_async_copy(b_ref, b_hbm, sems.at[1]),
        ]
        for copy in keep:
            copy.start()
        for j, w in enumerate((wk, wv)):
            cols = slice(j * width, (j + 1) * width)
            for lo, ref in ((0, t_ref), (half, b_ref)):
                span = slice(lo, lo + half)
                pair[span, cols] = (tot_ref[span, cols] + f32dot(ref[...], w[...])).astype(jnp.bfloat16)
            if j == 0:
                get.wait()
            for i in range(slots):
                block = jnp.clip(pick[i // MOST, i % MOST], 0, rows // BLK - 1)
                span = pl.ds(pl.multiple_of(block * BLK, BLK), BLK)
                pltpu.make_async_copy(pair.at[span, cols], send_hbm.at[i, :, cols], sends.at[j]).start()
        copy = pltpu.make_async_copy(pair, pair_hbm, sems.at[2])
        copy.start()
        keep.append(copy)
        for copy in keep:
            copy.wait()
        for j in range(2):
            sent = send_hbm.at[:, :, j * width : (j + 1) * width]
            pltpu.make_async_copy(sent, sent, sends.at[j]).wait()

    return pl.pallas_call(
        body,
        in_specs=[HBM, VMEM, VMEM, VMEM, VMEM, VMEM],
        out_specs=[HBM, HBM, HBM, HBM],
        out_shape=[
            in_hbm((rows, 2 * width), jnp.bfloat16),
            in_hbm((slots, BLK, 2 * width), jnp.bfloat16),
            in_hbm((half, feat), jnp.bfloat16),
            in_hbm((half, feat), jnp.bfloat16),
        ],
        scratch_shapes=[
            pltpu.SMEM((peers, HD), jnp.int32),
            pltpu.VMEM((rows, 2 * width), jnp.bfloat16),
            pltpu.SemaphoreType.DMA,
            pltpu.SemaphoreType.DMA((3,)),
            pltpu.SemaphoreType.DMA((2,)),
        ],
        compiler_params=params(),
        cost_estimate=cost(4 * rows * feat * width, 12 * feat * width),
        name="project_last",
    )(asked, top, bottom, wk_last, wv_last, total)


def project_query(where, own, left, right, top, bottom, w_query):
    rows, feat = own.shape
    half = top.shape[0]
    width = w_query.shape[1]

    def body(where_ref, o_ref, l_ref, r_ref, t_ref, b_ref, wo, wl, wr, wf, out_ref):
        for lo, far in ((0, t_ref), (half, b_ref)):
            span = slice(lo, lo + half)
            total = f32dot(o_ref[span, :], wo[...]) + f32dot(l_ref[span, :], wl[...])
            total = total + f32dot(r_ref[span, :], wr[...]) + f32dot(far[...], wf[...])
            out_ref[span, :] = total.astype(jnp.bfloat16)

    def chunk(k):
        return pl.BlockSpec((feat, width), lambda i, s: (s[k], 0))

    toks = pl.BlockSpec((rows, feat), lambda i, s: (0, 0))
    halves = pl.BlockSpec((half, feat), lambda i, s: (0, 0))
    return pl.pallas_call(
        body,
        grid_spec=pltpu.PrefetchScalarGridSpec(
            num_scalar_prefetch=1,
            grid=(1,),
            in_specs=[toks, toks, toks, halves, halves, chunk(0), chunk(1), chunk(2), chunk(3)],
            out_specs=pl.BlockSpec((rows, width), lambda i, s: (0, 0)),
        ),
        out_shape=in_hbm((rows, width), jnp.bfloat16),
        compiler_params=params(LARGE),
        cost_estimate=cost(8 * rows * feat * width, 16 * feat * width),
        name="project_query",
    )(where, *keep_in_hbm(own, left, right, top, bottom, w_query, w_query, w_query, w_query))


def plan(my_index, chosen, peers):
    rows, wide = chosen.shape
    slots = peers * MOST

    def body(me_ref, cho_ref, req_ref, mask_ref):
        me = me_ref[0]
        entries = cho_ref[...]
        peer = lax.broadcasted_iota(jnp.int32, (peers, wide), 0)
        low = jnp.full((peers, wide), rows, jnp.int32)
        high = jnp.full((peers, wide), -1, jnp.int32)
        for r in range(rows):
            entry = jnp.broadcast_to(entries[r : r + 1, :], (peers, wide))
            block = entry - peer * rows
            mine = (block >= 0) & (block < rows)
            low = jnp.where(mine, jnp.minimum(low, block), low)
            high = jnp.where(mine, jnp.maximum(high, block), high)
        low = jnp.min(low, axis=1, keepdims=True)
        high = jnp.max(high, axis=1, keepdims=True)
        far = lax.broadcasted_iota(jnp.int32, (peers, 1), 0) != me
        first = jnp.where(far & (low < rows), low, -1)
        second = jnp.where(far & (high > low), high, -1)
        lane = lax.broadcasted_iota(jnp.int32, (peers, HD), 1)
        req_ref[...] = jnp.where(lane == 0, first, jnp.where(lane == 1, second, -1))
        at = lax.broadcasted_iota(jnp.int32, (peers, HD), 0)
        named = jnp.where(lane == MOST * at, first, jnp.where(lane == MOST * at + 1, second, -1))
        named = jnp.where(named >= 0, named + at * rows, -1)
        ids = jnp.max(named, axis=0, keepdims=True)
        slot = lax.broadcasted_iota(jnp.int32, (1, HD), 1)
        own = (slot >= slots) & (slot < slots + rows)
        ids = jnp.where(own, me * rows + slot - slots, ids)
        seen = entries[:, :1] == ids
        for k in range(1, wide):
            seen = seen | (entries[:, k : k + 1] == ids)
        bias = jnp.where(seen, 0.0, NEG)
        for r in range(rows):
            mask_ref[r * BLK : (r + 1) * BLK, :] = jnp.broadcast_to(bias[r : r + 1, :], (BLK, HD)).astype(jnp.bfloat16)

    return pl.pallas_call(
        body,
        grid_spec=pltpu.PrefetchScalarGridSpec(
            num_scalar_prefetch=1,
            grid=(1,),
            in_specs=[pl.BlockSpec((rows, wide), lambda i, s: (0, 0))],
            out_specs=[
                pl.BlockSpec((peers, HD), lambda i, s: (0, 0)),
                pl.BlockSpec((rows * BLK, HD), lambda i, s: (0, 0)),
            ],
        ),
        out_shape=[in_hbm((peers, HD), jnp.int32), in_hbm((rows * BLK, HD), jnp.bfloat16)],
        compiler_params=params(),
        cost_estimate=cost(1000000, 200000),
        name="plan",
    )(my_index, chosen)


def one_hot(rows, first_slot):
    slot = lax.broadcasted_iota(jnp.int32, (rows, HD), 0) // BLK + first_slot
    return (slot == lax.broadcasted_iota(jnp.int32, (rows, HD), 1)).astype(jnp.bfloat16)


def scores_of(query, keys):
    return lax.dot_general(query, keys, (((1,), (1,)), ((), ())), preferred_element_type=jnp.float32)


def attend_own(query, pair, mask, first_slot):
    rows, width = query.shape
    heads = width // HD
    scale = HD ** (-0.5) * LOG2E
    tile = 256

    def body(q_ref, k_ref, v_ref, mask_ref, high_ref, tot_ref, sum_ref):
        keys = jnp.concatenate([k_ref[...], one_hot(rows, first_slot)], axis=1)
        values = jnp.concatenate([v_ref[...], jnp.ones_like(v_ref)], axis=1)
        for lo in range(0, rows, tile):
            span = slice(lo, lo + tile)
            count = lo + tile
            wide = jnp.concatenate([q_ref[span, :], mask_ref[span, :]], axis=1)
            scores = scores_of(wide, keys[:count])
            row = lax.broadcasted_iota(jnp.int32, scores.shape, 0) + lo
            col = lax.broadcasted_iota(jnp.int32, scores.shape, 1)
            scores = jnp.where(col <= row, scores, NEG)
            high = jnp.max(scores, axis=1, keepdims=True)
            weights = jnp.exp2((scores - high) * scale).astype(jnp.bfloat16)
            summed = f32dot(weights, values[:count])
            high_ref[span, :] = jnp.broadcast_to(high, (tile, HD))
            tot_ref[span, :] = summed[:, HD:]
            sum_ref[span, :] = summed[:, :HD]

    column = pl.BlockSpec((rows, HD), lambda h: (0, h))
    return pl.pallas_call(
        body,
        grid=(heads,),
        in_specs=[
            column,
            column,
            pl.BlockSpec((rows, HD), lambda h: (0, heads + h)),
            pl.BlockSpec((rows, HD), lambda h: (0, 0)),
        ],
        out_specs=[column, column, column],
        out_shape=[in_hbm((rows, width), jnp.float32)] * 3,
        compiler_params=params(LARGE),
        cost_estimate=cost(8 * rows * rows * width, 16 * rows * width, rows * rows * heads),
        name="attend_own",
    )(query, pair, pair, mask)


def attend_far(where, query, got, mask, high, total, summed, carried):
    rows, width = query.shape
    heads = width // HD
    count = got.shape[0]
    scale = HD ** (-0.5) * LOG2E
    parts = where.shape[0]
    tile = rows // parts
    pairs = ((3, 1), (2, 0))

    def body(where_ref, q_ref, k_ref, v_ref, mask_ref, high_ref, tot_ref, sum_ref, *rest):
        pieces = len(carried)
        copies = [
            pltpu.make_async_copy(rest[k], rest[pieces + parts + k], rest[-1].at[k]) for k in range(pieces)
        ]
        outs = rest[pieces : pieces + parts]
        keys, values = rest[-3:-1]

        @pl.when(pl.program_id(0) == 1)
        def _():
            for copy in copies:
                copy.start()

        @pl.when(pl.program_id(0) == 0)
        def _():
            keys[:, HD:] = one_hot(count, 0)
            values[:, HD:] = jnp.ones_like(v_ref)

        keys[:, :HD] = k_ref[...]
        values[:, :HD] = v_ref[...]

        def rows_of(ref, parts_at):
            spans = [pl.ds(pl.multiple_of(where_ref[p] * tile, tile), tile) for p in parts_at]
            return jnp.concatenate([ref[span, :] for span in spans], axis=0)

        def scores_at(parts_at):
            wide = jnp.concatenate([rows_of(q_ref, parts_at), rows_of(mask_ref, parts_at)], axis=1)
            return scores_of(wide, keys[...])

        later = scores_at(pairs[0])
        for i, parts_at in enumerate(pairs):
            scores = later
            if i + 1 < len(pairs):
                later = scores_at(pairs[i + 1])
            own = rows_of(high_ref, parts_at)
            top = jnp.maximum(jnp.max(scores, axis=1, keepdims=True), own[:, :1])
            weights = jnp.exp2((scores - top) * scale).astype(jnp.bfloat16)
            far = f32dot(weights, values[...])
            keep = jnp.exp2((own - top) * scale)
            result = far[:, :HD] + keep * rows_of(sum_ref, parts_at)
            result = (result / (far[:, HD:] + keep * rows_of(tot_ref, parts_at))).astype(jnp.bfloat16)
            for k, part in enumerate(parts_at):
                outs[part][...] = result[k * tile : (k + 1) * tile]

        @pl.when(pl.program_id(0) == heads - 1)
        def _():
            for copy in copies:
                copy.wait()

    column = pl.BlockSpec((rows, HD), lambda h, s: (0, h))
    return pl.pallas_call(
        body,
        grid_spec=pltpu.PrefetchScalarGridSpec(
            num_scalar_prefetch=1,
            grid=(heads,),
            in_specs=[
                column,
                pl.BlockSpec((count, HD), lambda h, s: (0, h)),
                pl.BlockSpec((count, HD), lambda h, s: (0, heads + h)),
                pl.BlockSpec((rows, HD), lambda h, s: (0, 0)),
                column,
                column,
                column,
            ]
            + [HBM] * len(carried),
            out_specs=[pl.BlockSpec((tile, HD), lambda h, s: (0, h))] * parts + [VMEM] * len(carried),
            scratch_shapes=[pltpu.VMEM((count, 2 * HD), jnp.bfloat16)] * 2
            + [pltpu.SemaphoreType.DMA((len(carried),))],
        ),
        out_shape=[jax.ShapeDtypeStruct((tile, width), jnp.bfloat16)] * parts
        + [in_vmem(w.shape, w.dtype) for w in carried],
        compiler_params=params(),
        cost_estimate=cost(8 * rows * count * width, 4 * count * width, rows * count * heads),
        name="attend_far",
    )(where, *keep_in_hbm(query), got, got, *keep_in_hbm(mask, high, total, summed, *carried))


def mix(core, attended, w_own, mine, other):
    rows, width = attended[0].shape
    span = mine[0].shape[1]
    part = mine[2].shape[1]

    def body(core_ref, own_ref, l_ref, r_ref, f_ref, w_ref, *rest):
        out_hbm, out_ref, sems = rest[8:]
        copies = []
        for side, pieces in enumerate((rest[:4], rest[4:8])):
            at = pl.multiple_of((core_ref[0] if side == 0 else 1 - core_ref[0]) * span, span)
            total = f32dot(own_ref[...], w_ref[:, pl.ds(at, span)])
            total = total + f32dot(l_ref[...], pieces[0][...]) + f32dot(r_ref[...], pieces[1][...])
            for k in range(2):
                to = slice(k * part, (k + 1) * part)
                value = total[:, to] + f32dot(f_ref[...], pieces[2 + k][...])
                out_ref[side, :, to] = value.astype(jnp.bfloat16)
            copies.append(pltpu.make_async_copy(out_ref.at[side], out_hbm.at[:, pl.ds(at, span)], sems.at[side]))
            copies[-1].start()
        for copy in copies:
            copy.wait()

    args = (*attended, w_own, *mine, *other)
    return pl.pallas_call(
        body,
        in_specs=[SMEM] + [VMEM] * len(args),
        out_specs=HBM,
        out_shape=in_hbm((rows, 2 * span), jnp.bfloat16),
        scratch_shapes=[pltpu.VMEM((2, rows, span), jnp.bfloat16), pltpu.SemaphoreType.DMA((2,))],
        compiler_params=params(),
        cost_estimate=cost(16 * rows * width * span, 16 * width * span),
        name="mix",
    )(core, *args)


def local(tokens, w_query, w_key, w_value, w_out, chosen):
    tok_rows = tokens.shape[0]
    width = w_query.shape[1]
    half = tok_rows // 2
    peers = lax.axis_size(KV)
    tp = lax.axis_index("tp")
    count = lax.axis_size("tp")
    where = jnp.stack([tp, (tp + count - 1) % count, (tp + 1) % count, (tp + 2) % count]).astype(jnp.int32)
    me = jnp.reshape(lax.axis_index(KV), (1,)).astype(jnp.int32)
    core = jnp.reshape(lax.axis_index("kv_2"), (1,)).astype(jnp.int32)
    tokens, where, me, core = lax.optimization_barrier((tokens, where, me, core))

    left = shifted(tokens, "tp", 1)
    right = shifted(tokens, "tp", -1)
    request, mask = plan(me, chosen, peers)
    asked = lax.all_to_all(request, KV, 0, 0, tiled=True)
    left, right, request, mask = lax.optimization_barrier((left, right, request, mask))

    top = shifted(left[:half], "tp", 1)
    bottom = shifted(right[half:], "tp", -1)
    total, wk_last, wv_last, left, right = project_near(where, tokens, left, right, w_key, w_value)
    pair, send, top, bottom = project_last(asked, top, bottom, wk_last, wv_last, total)
    w_mine, send = lax.optimization_barrier((w_out, send))
    got = lax.all_to_all(send, KV, split_axis=0, concat_axis=0, tiled=True)

    span = w_out.shape[1] // 2
    part = span // 2
    piece = lax.dynamic_slice_in_dim(w_mine, core[0] * span, span, axis=1)
    w_left = shifted(piece, "tp", 1)
    w_right = shifted(piece, "tp", -1)
    w_low = shifted(w_left[:, :part], "tp", 1)
    w_high = shifted(w_right[:, part:], "tp", -1)
    mine = (w_left, w_right, w_low, w_high)
    other = tuple(shifted(w, "kv_2", 1) for w in mine)

    query = project_query(where, tokens, left, right, top, bottom, w_query)
    high, totals, summed = attend_own(query, pair, mask, peers * MOST)
    weights = (w_out, *mine, *other)
    outs = attend_far(where, query, got.reshape(-1, 2 * width), mask, high, totals, summed, weights)
    attended = (outs[0], shifted(outs[2], "tp", 1), shifted(outs[1], "tp", -1), shifted(outs[3], "tp", 2))
    return mix(core, attended, outs[4], outs[5:9], outs[9:])


def solution(mesh):
    finer = Mesh(mesh.devices.reshape(4, 4, 2, mesh.shape["tp"]), ("kv_0", "kv_1", "kv_2", "tp"))
    placed = (P(KV, "tp"), P(None, "tp"), P(None, "tp"), P(None, "tp"), P("tp", None), P(KV, None))

    return jax.shard_map(local, mesh=finer, in_specs=placed, out_specs=P(KV_TP, None), check_vma=False)
```

```python
import jax
import jax.numpy as jnp
from jax import lax
from jax.experimental import pallas as pl
from jax.experimental.pallas import tpu as pltpu
from jax.sharding import Mesh
from jax.sharding import PartitionSpec as P


HD = 128
BLK = 32
MOST = 2
KV = ("kv_0", "kv_1", "kv_2")
KV_TP = ("kv_0", "kv_1", "kv_2", "tp")
NEG = -1e30
LOG2E = 1.4426950408889634
SMALL = 24 * 1024 * 1024
HBM = pl.BlockSpec(memory_space=pltpu.HBM)
VMEM = pl.BlockSpec(memory_space=pltpu.VMEM)
SMEM = pl.BlockSpec(memory_space=pltpu.SMEM)


def params(limit=SMALL):
    return pltpu.CompilerParams(vmem_limit_bytes=limit)


def in_hbm(shape, dtype):
    return pltpu.HBM(shape, dtype)


def in_vmem(shape, dtype):
    return pltpu.VMEM(shape, dtype)


def cost(flops, nbytes, exps=0):
    return pl.CostEstimate(flops=int(flops), bytes_accessed=int(nbytes), transcendentals=int(exps))


def keep_in_hbm(*arrays):
    return tuple(pltpu.with_memory_space_constraint(a, pltpu.HBM) for a in arrays)


def f32dot(a, b):
    return jnp.dot(a, b, preferred_element_type=jnp.float32)


def shifted(array, axis, by):
    count = lax.axis_size(axis)
    return lax.ppermute(array, axis, [(i, (i + by) % count) for i in range(count)])


def project_near(where, core, own, left, right, w_key, w_value, w_out):
    rows, feat = own.shape
    width = w_key.shape[1]
    chunks = where.shape[0]
    part = w_out.shape[1] // 4

    def body(where_ref, core_ref, own_hbm, l_ref, r_ref, wk_hbm, wv_hbm, w_hbm, *rest):
        tot_ref, wk_last, wv_last, l_hbm, r_hbm, low_ref, high_ref, own_ref, chunk_refs, sems = rest
        copies = []

        def fetch(src, dst):
            copies.append(pltpu.make_async_copy(src, dst, sems.at[len(copies)]))
            copies[-1].start()
            return copies[-1]

        own_copy = fetch(own_hbm, own_ref)
        pieces = []
        for k in range(chunks - 1):
            span = pl.ds(pl.multiple_of(where_ref[k] * feat, feat), feat)
            for j, w in enumerate((wk_hbm, wv_hbm)):
                pieces.append(fetch(w.at[span, :], chunk_refs.at[k, j]))
        span = pl.ds(pl.multiple_of(where_ref[chunks - 1] * feat, feat), feat)
        last = [fetch(wk_hbm.at[span, :], wk_last), fetch(wv_hbm.at[span, :], wv_last)]
        last += [fetch(l_ref, l_hbm), fetch(r_ref, r_hbm)]
        for k, ref in enumerate((low_ref, high_ref)):
            at = pl.multiple_of((2 * core_ref[0] + k) * part, part)
            last.append(fetch(w_hbm.at[:, pl.ds(at, part)], ref))
        own_copy.wait()
        for copy in pieces:
            copy.wait()
        for j in range(2):
            total = f32dot(own_ref[...], chunk_refs[0, j]) + f32dot(l_ref[...], chunk_refs[1, j])
            tot_ref[:, j * width : (j + 1) * width] = total + f32dot(r_ref[...], chunk_refs[2, j])
        for copy in last:
            copy.wait()

    chunk = (feat, width)
    return pl.pallas_call(
        body,
        in_specs=[SMEM, SMEM, HBM, VMEM, VMEM, HBM, HBM, HBM],
        out_specs=[VMEM, VMEM, VMEM, HBM, HBM, VMEM, VMEM],
        out_shape=[
            in_vmem((rows, 2 * width), jnp.float32),
            in_vmem(chunk, jnp.bfloat16),
            in_vmem(chunk, jnp.bfloat16),
            in_hbm((rows, feat), jnp.bfloat16),
            in_hbm((rows, feat), jnp.bfloat16),
            in_vmem((w_out.shape[0], part), jnp.bfloat16),
            in_vmem((w_out.shape[0], part), jnp.bfloat16),
        ],
        scratch_shapes=[
            pltpu.VMEM((rows, feat), jnp.bfloat16),
            pltpu.VMEM((chunks - 1, 2, feat, width), jnp.bfloat16),
            pltpu.SemaphoreType.DMA((2 * chunks + 5,)),
        ],
        compiler_params=params(),
        cost_estimate=cost(12 * rows * feat * width, 20 * feat * width),
        name="project_near",
    )(where, core, *keep_in_hbm(own), left, right, *keep_in_hbm(w_key, w_value, w_out))


def project_last(asked, top, bottom, wk_last, wv_last, total):
    half, feat = top.shape
    rows = 2 * half
    width = wk_last.shape[1]
    peers = asked.shape[0]
    slots = peers * MOST

    def body(asked_hbm, t_ref, b_ref, wk, wv, tot_ref, pair_hbm, send_hbm, t_hbm, b_hbm, pick, pair, sem, sems, sends):
        get = pltpu.make_async_copy(asked_hbm, pick, sem)
        get.start()
        keep = [
            pltpu.make_async_copy(t_ref, t_hbm, sems.at[0]),
            pltpu.make_async_copy(b_ref, b_hbm, sems.at[1]),
        ]
        for copy in keep:
            copy.start()
        for j, w in enumerate((wk, wv)):
            cols = slice(j * width, (j + 1) * width)
            for lo, ref in ((0, t_ref), (half, b_ref)):
                span = slice(lo, lo + half)
                pair[span, cols] = (tot_ref[span, cols] + f32dot(ref[...], w[...])).astype(jnp.bfloat16)
            if j == 0:
                get.wait()
            for i in range(slots):
                block = jnp.clip(pick[i // MOST, i % MOST], 0, rows // BLK - 1)
                span = pl.ds(pl.multiple_of(block * BLK, BLK), BLK)
                pltpu.make_async_copy(pair.at[span, cols], send_hbm.at[i, :, cols], sends.at[j]).start()
        copy = pltpu.make_async_copy(pair, pair_hbm, sems.at[2])
        copy.start()
        keep.append(copy)
        for copy in keep:
            copy.wait()
        for j in range(2):
            sent = send_hbm.at[:, :, j * width : (j + 1) * width]
            pltpu.make_async_copy(sent, sent, sends.at[j]).wait()

    return pl.pallas_call(
        body,
        in_specs=[HBM, VMEM, VMEM, VMEM, VMEM, VMEM],
        out_specs=[HBM, HBM, HBM, HBM],
        out_shape=[
            in_hbm((rows, 2 * width), jnp.bfloat16),
            in_hbm((slots, BLK, 2 * width), jnp.bfloat16),
            in_hbm((half, feat), jnp.bfloat16),
            in_hbm((half, feat), jnp.bfloat16),
        ],
        scratch_shapes=[
            pltpu.SMEM((peers, HD), jnp.int32),
            pltpu.VMEM((rows, 2 * width), jnp.bfloat16),
            pltpu.SemaphoreType.DMA,
            pltpu.SemaphoreType.DMA((3,)),
            pltpu.SemaphoreType.DMA((2,)),
        ],
        compiler_params=params(),
        cost_estimate=cost(4 * rows * feat * width, 12 * feat * width),
        name="project_last",
    )(asked, top, bottom, wk_last, wv_last, total)


def project_query(where, own, left, right, top, bottom, w_query):
    rows, feat = own.shape
    half = top.shape[0]
    width = w_query.shape[1]

    def body(where_ref, o_ref, l_ref, r_ref, t_ref, b_ref, wo, wl, wr, wf, out_ref):
        for lo, far in ((0, t_ref), (half, b_ref)):
            span = slice(lo, lo + half)
            total = f32dot(o_ref[span, :], wo[...]) + f32dot(l_ref[span, :], wl[...])
            total = total + f32dot(r_ref[span, :], wr[...]) + f32dot(far[...], wf[...])
            out_ref[span, :] = total.astype(jnp.bfloat16)

    def chunk(k):
        return pl.BlockSpec((feat, width), lambda i, s: (s[k], 0))

    toks = pl.BlockSpec((rows, feat), lambda i, s: (0, 0))
    halves = pl.BlockSpec((half, feat), lambda i, s: (0, 0))
    return pl.pallas_call(
        body,
        grid_spec=pltpu.PrefetchScalarGridSpec(
            num_scalar_prefetch=1,
            grid=(1,),
            in_specs=[toks, toks, toks, halves, halves, chunk(0), chunk(1), chunk(2), chunk(3)],
            out_specs=pl.BlockSpec((rows, width), lambda i, s: (0, 0)),
        ),
        out_shape=in_vmem((rows, width), jnp.bfloat16),
        compiler_params=params(),
        cost_estimate=cost(8 * rows * feat * width, 16 * feat * width),
        name="project_query",
    )(where, *keep_in_hbm(own, left, right, top, bottom, w_query, w_query, w_query, w_query))


def plan(my_index, chosen, peers):
    rows, wide = chosen.shape
    slots = peers * MOST

    def body(me_ref, cho_ref, req_ref, mask_ref):
        me = me_ref[0]
        entries = cho_ref[...]
        peer = lax.broadcasted_iota(jnp.int32, (peers, wide), 0)
        low = jnp.full((peers, wide), rows, jnp.int32)
        high = jnp.full((peers, wide), -1, jnp.int32)
        for r in range(rows):
            entry = jnp.broadcast_to(entries[r : r + 1, :], (peers, wide))
            block = entry - peer * rows
            mine = (block >= 0) & (block < rows)
            low = jnp.where(mine, jnp.minimum(low, block), low)
            high = jnp.where(mine, jnp.maximum(high, block), high)
        low = jnp.min(low, axis=1, keepdims=True)
        high = jnp.max(high, axis=1, keepdims=True)
        far = lax.broadcasted_iota(jnp.int32, (peers, 1), 0) != me
        first = jnp.where(far & (low < rows), low, -1)
        second = jnp.where(far & (high > low), high, -1)
        lane = lax.broadcasted_iota(jnp.int32, (peers, HD), 1)
        req_ref[...] = jnp.where(lane == 0, first, jnp.where(lane == 1, second, -1))
        at = lax.broadcasted_iota(jnp.int32, (peers, HD), 0)
        named = jnp.where(lane == MOST * at, first, jnp.where(lane == MOST * at + 1, second, -1))
        named = jnp.where(named >= 0, named + at * rows, -1)
        ids = jnp.max(named, axis=0, keepdims=True)
        slot = lax.broadcasted_iota(jnp.int32, (1, HD), 1)
        own = (slot >= slots) & (slot < slots + rows)
        ids = jnp.where(own, me * rows + slot - slots, ids)
        seen = entries[:, :1] == ids
        for k in range(1, wide):
            seen = seen | (entries[:, k : k + 1] == ids)
        bias = jnp.where(seen, 0.0, NEG)
        for r in range(rows):
            mask_ref[r * BLK : (r + 1) * BLK, :] = jnp.broadcast_to(bias[r : r + 1, :], (BLK, HD)).astype(jnp.bfloat16)

    return pl.pallas_call(
        body,
        grid_spec=pltpu.PrefetchScalarGridSpec(
            num_scalar_prefetch=1,
            grid=(1,),
            in_specs=[pl.BlockSpec((rows, wide), lambda i, s: (0, 0))],
            out_specs=[
                pl.BlockSpec((peers, HD), lambda i, s: (0, 0)),
                pl.BlockSpec((rows * BLK, HD), lambda i, s: (0, 0)),
            ],
        ),
        out_shape=[in_hbm((peers, HD), jnp.int32), in_hbm((rows * BLK, HD), jnp.bfloat16)],
        compiler_params=params(),
        cost_estimate=cost(1000000, 200000),
        name="plan",
    )(my_index, chosen)


def one_hot(rows, first_slot):
    slot = lax.broadcasted_iota(jnp.int32, (rows, HD), 0) // BLK + first_slot
    return (slot == lax.broadcasted_iota(jnp.int32, (rows, HD), 1)).astype(jnp.bfloat16)


def scores_of(query, keys):
    return lax.dot_general(query, keys, (((1,), (1,)), ((), ())), preferred_element_type=jnp.float32)


def attend_own(query, pair, mask, first_slot):
    rows, width = query.shape
    heads = width // HD
    scale = HD ** (-0.5) * LOG2E
    tile = 256

    def body(q_ref, k_ref, v_ref, mask_ref, high_ref, tot_ref, sum_ref):
        keys = jnp.concatenate([k_ref[...], one_hot(rows, first_slot)], axis=1)
        values = jnp.concatenate([v_ref[...], jnp.ones_like(v_ref)], axis=1)
        for lo in range(0, rows, tile):
            span = slice(lo, lo + tile)
            count = lo + tile
            wide = jnp.concatenate([q_ref[span, :], mask_ref[span, :]], axis=1)
            scores = scores_of(wide, keys[:count])
            row = lax.broadcasted_iota(jnp.int32, scores.shape, 0) + lo
            col = lax.broadcasted_iota(jnp.int32, scores.shape, 1)
            scores = jnp.where(col <= row, scores, NEG)
            high = jnp.max(scores, axis=1, keepdims=True)
            weights = jnp.exp2((scores - high) * scale).astype(jnp.bfloat16)
            summed = f32dot(weights, values[:count])
            high_ref[span, :] = jnp.broadcast_to(high, (tile, HD))
            tot_ref[span, :] = summed[:, HD:]
            sum_ref[span, :] = summed[:, :HD]

    column = pl.BlockSpec((rows, HD), lambda h: (0, h))
    return pl.pallas_call(
        body,
        grid=(heads,),
        in_specs=[
            column,
            column,
            pl.BlockSpec((rows, HD), lambda h: (0, heads + h)),
            pl.BlockSpec((rows, HD), lambda h: (0, 0)),
        ],
        out_specs=[column, column, column],
        out_shape=[in_hbm((rows, width), jnp.float32)] * 3,
        compiler_params=params(),
        cost_estimate=cost(8 * rows * rows * width, 16 * rows * width, rows * rows * heads),
        name="attend_own",
    )(query, *keep_in_hbm(pair, pair, mask))


def attend_far(where, query, got, mask, high, total, summed, carried):
    rows, width = query.shape
    heads = width // HD
    count = got.shape[0]
    scale = HD ** (-0.5) * LOG2E
    parts = where.shape[0]
    tile = rows // parts
    pairs = ((3, 1), (2, 0))

    def body(where_ref, q_ref, k_ref, v_ref, mask_ref, high_ref, tot_ref, sum_ref, *rest):
        pieces = len(carried)
        copies = [
            pltpu.make_async_copy(rest[k], rest[pieces + parts + k], rest[-1].at[k]) for k in range(pieces)
        ]
        outs = rest[pieces : pieces + parts]
        keys, values = rest[-3:-1]

        @pl.when(pl.program_id(0) == 1)
        def _():
            for copy in copies:
                copy.start()

        @pl.when(pl.program_id(0) == 0)
        def _():
            keys[:, HD:] = one_hot(count, 0)
            values[:, HD:] = jnp.ones_like(v_ref)

        keys[:, :HD] = k_ref[...]
        values[:, :HD] = v_ref[...]

        def rows_of(ref, parts_at):
            spans = [pl.ds(pl.multiple_of(where_ref[p] * tile, tile), tile) for p in parts_at]
            return jnp.concatenate([ref[span, :] for span in spans], axis=0)

        def scores_at(parts_at):
            wide = jnp.concatenate([rows_of(q_ref, parts_at), rows_of(mask_ref, parts_at)], axis=1)
            return scores_of(wide, keys[...])

        later = scores_at(pairs[0])
        for i, parts_at in enumerate(pairs):
            scores = later
            if i + 1 < len(pairs):
                later = scores_at(pairs[i + 1])
            own = rows_of(high_ref, parts_at)
            top = jnp.maximum(jnp.max(scores, axis=1, keepdims=True), own[:, :1])
            weights = jnp.exp2((scores - top) * scale).astype(jnp.bfloat16)
            far = f32dot(weights, values[...])
            keep = jnp.exp2((own - top) * scale)
            result = far[:, :HD] + keep * rows_of(sum_ref, parts_at)
            result = (result / (far[:, HD:] + keep * rows_of(tot_ref, parts_at))).astype(jnp.bfloat16)
            for k, part in enumerate(parts_at):
                outs[part][...] = result[k * tile : (k + 1) * tile]

        @pl.when(pl.program_id(0) == heads - 1)
        def _():
            for copy in copies:
                copy.wait()

    column = pl.BlockSpec((rows, HD), lambda h, s: (0, h))
    return pl.pallas_call(
        body,
        grid_spec=pltpu.PrefetchScalarGridSpec(
            num_scalar_prefetch=1,
            grid=(heads,),
            in_specs=[
                column,
                pl.BlockSpec((count, HD), lambda h, s: (0, h)),
                pl.BlockSpec((count, HD), lambda h, s: (0, heads + h)),
                pl.BlockSpec((rows, HD), lambda h, s: (0, 0)),
                column,
                column,
                column,
            ]
            + [HBM] * len(carried),
            out_specs=[pl.BlockSpec((tile, HD), lambda h, s: (0, h))] * parts + [VMEM] * len(carried),
            scratch_shapes=[pltpu.VMEM((count, 2 * HD), jnp.bfloat16)] * 2
            + [pltpu.SemaphoreType.DMA((len(carried),))],
        ),
        out_shape=[jax.ShapeDtypeStruct((tile, width), jnp.bfloat16)] * parts
        + [in_vmem(w.shape, w.dtype) for w in carried],
        compiler_params=params(),
        cost_estimate=cost(8 * rows * count * width, 4 * count * width, rows * count * heads),
        name="attend_far",
    )(where, query, got, got, *keep_in_hbm(mask, high, total, summed, *carried))


def mix(core, attended, w_own, mine, other):
    rows, width = attended[0].shape
    part = mine[0].shape[1]

    def body(core_ref, *rest):
        own_ref, far_refs, w_ref, pieces = rest[0], rest[1:4], rest[4], (rest[5:11], rest[11:17])
        out_hbm, out_ref, sems = rest[17:]
        copies = []
        for side in range(2):
            base = (core_ref[0] if side == 0 else 1 - core_ref[0]) * 2
            for k in range(2):
                span = pl.ds(pl.multiple_of((base + k) * part, part), part)
                total = f32dot(own_ref[...], w_ref[:, span])
                for g in range(3):
                    total = total + f32dot(far_refs[g][...], pieces[side][2 * g + k][...])
                at = 2 * side + k
                out_ref[at] = total.astype(jnp.bfloat16)
                copies.append(pltpu.make_async_copy(out_ref.at[at], out_hbm.at[:, span], sems.at[at]))
                copies[-1].start()
        for copy in copies:
            copy.wait()

    args = (*attended, w_own, *mine, *other)
    return pl.pallas_call(
        body,
        in_specs=[SMEM] + [VMEM] * len(args),
        out_specs=HBM,
        out_shape=in_hbm((rows, 4 * part), jnp.bfloat16),
        scratch_shapes=[pltpu.VMEM((4, rows, part), jnp.bfloat16), pltpu.SemaphoreType.DMA((4,))],
        compiler_params=params(),
        cost_estimate=cost(32 * rows * width * part, 32 * width * part),
        name="mix",
    )(core, *args)


def local(tokens, w_query, w_key, w_value, w_out, chosen):
    tok_rows = tokens.shape[0]
    width = w_query.shape[1]
    half = tok_rows // 2
    peers = lax.axis_size(KV)
    tp = lax.axis_index("tp")
    count = lax.axis_size("tp")
    where = jnp.stack([tp, (tp + count - 1) % count, (tp + 1) % count, (tp + 2) % count]).astype(jnp.int32)
    me = jnp.reshape(lax.axis_index(KV), (1,)).astype(jnp.int32)
    core = jnp.reshape(lax.axis_index("kv_2"), (1,)).astype(jnp.int32)
    tokens, where, me, core = lax.optimization_barrier((tokens, where, me, core))

    left = shifted(tokens, "tp", 1)
    right = shifted(tokens, "tp", -1)
    request, mask = plan(me, chosen, peers)
    asked = lax.all_to_all(request, KV, 0, 0, tiled=True)
    left, right, request, mask = lax.optimization_barrier((left, right, request, mask))

    top = shifted(left[:half], "tp", 1)
    bottom = shifted(right[half:], "tp", -1)
    total, wk_last, wv_last, left, right, low, high_part = project_near(
        where, core, tokens, left, right, w_key, w_value, w_out
    )
    pair, send, top, bottom = project_last(asked, top, bottom, wk_last, wv_last, total)
    low, high_part, send = lax.optimization_barrier((low, high_part, send))
    got = lax.all_to_all(send, KV, split_axis=0, concat_axis=0, tiled=True)

    left_low = shifted(low, "tp", 1)
    right_high = shifted(high_part, "tp", -1)
    left_high = shifted(high_part, "tp", 1)
    right_low = shifted(low, "tp", -1)
    far_low = shifted(left_low, "tp", 1)
    far_high = shifted(right_high, "tp", -1)
    mine = (left_low, left_high, right_low, right_high, far_low, far_high)
    other = tuple(shifted(w, "kv_2", 1) for w in mine)

    query = project_query(where, tokens, left, right, top, bottom, w_query)
    high, totals, summed = attend_own(query, pair, mask, peers * MOST)
    weights = (w_out, *mine, *other)
    outs = attend_far(where, query, got.reshape(-1, 2 * width), mask, high, totals, summed, weights)
    attended = (outs[0], shifted(outs[2], "tp", 1), shifted(outs[1], "tp", -1), shifted(outs[3], "tp", 2))
    return mix(core, attended, outs[4], outs[5:11], outs[11:])


def solution(mesh):
    finer = Mesh(mesh.devices.reshape(4, 4, 2, mesh.shape["tp"]), ("kv_0", "kv_1", "kv_2", "tp"))
    placed = (P(KV, "tp"), P(None, "tp"), P(None, "tp"), P(None, "tp"), P("tp", None), P(KV, None))

    return jax.shard_map(local, mesh=finer, in_specs=placed, out_specs=P(KV_TP, None), check_vma=False)
```

```python
import jax
import jax.numpy as jnp
from jax import lax
from jax.experimental import pallas as pl
from jax.experimental.pallas import tpu as pltpu
from jax.sharding import Mesh
from jax.sharding import PartitionSpec as P


HD = 128
BLK = 32
MOST = 2
KV = ("kv_0", "kv_1", "kv_2")
KV_TP = ("kv_0", "kv_1", "kv_2", "tp")
NEG = -1e30
SCALE = HD ** (-0.5) * 1.4426950408889634
SMALL = 24 * 1024 * 1024
HBM = pl.BlockSpec(memory_space=pltpu.HBM)
VMEM = pl.BlockSpec(memory_space=pltpu.VMEM)
SMEM = pl.BlockSpec(memory_space=pltpu.SMEM)


def params(limit=SMALL):
    return pltpu.CompilerParams(vmem_limit_bytes=limit)


def in_hbm(shape, dtype):
    return pltpu.HBM(shape, dtype)


def in_vmem(shape, dtype):
    return pltpu.VMEM(shape, dtype)


def cost(flops, nbytes, exps=0):
    return pl.CostEstimate(flops=int(flops), bytes_accessed=int(nbytes), transcendentals=int(exps))


def keep_in_hbm(*arrays):
    return tuple(pltpu.with_memory_space_constraint(a, pltpu.HBM) for a in arrays)


def f32dot(a, b):
    return jnp.dot(a, b, preferred_element_type=jnp.float32)


def shifted(array, axis, by):
    count = lax.axis_size(axis)
    return lax.ppermute(array, axis, [(i, (i + by) % count) for i in range(count)])


def project_near(where, core, own, left, right, w_key, w_value, w_out):
    rows, feat = own.shape
    width = w_key.shape[1]
    chunks = where.shape[0]
    part = w_out.shape[1] // 4

    def body(where_ref, core_ref, own_hbm, l_ref, r_ref, wk_hbm, wv_hbm, w_hbm, *rest):
        tot_ref, wk_last, wv_last, l_hbm, r_hbm, low_ref, high_ref, own_ref, chunk_refs, sems = rest
        copies = []

        def fetch(src, dst):
            copies.append(pltpu.make_async_copy(src, dst, sems.at[len(copies)]))
            copies[-1].start()
            return copies[-1]

        own_copy = fetch(own_hbm, own_ref)
        pieces = []
        for k in range(chunks - 1):
            span = pl.ds(pl.multiple_of(where_ref[k] * feat, feat), feat)
            for j, w in enumerate((wk_hbm, wv_hbm)):
                pieces.append(fetch(w.at[span, :], chunk_refs.at[k, j]))
        span = pl.ds(pl.multiple_of(where_ref[chunks - 1] * feat, feat), feat)
        last = [fetch(wk_hbm.at[span, :], wk_last), fetch(wv_hbm.at[span, :], wv_last)]
        last += [fetch(l_ref, l_hbm), fetch(r_ref, r_hbm)]
        for k, ref in enumerate((low_ref, high_ref)):
            at = pl.multiple_of((2 * core_ref[0] + k) * part, part)
            last.append(fetch(w_hbm.at[:, pl.ds(at, part)], ref))
        own_copy.wait()
        for copy in pieces:
            copy.wait()
        for j in range(2):
            total = f32dot(own_ref[...], chunk_refs[0, j]) + f32dot(l_ref[...], chunk_refs[1, j])
            tot_ref[:, j * width : (j + 1) * width] = total + f32dot(r_ref[...], chunk_refs[2, j])
        for copy in last:
            copy.wait()

    chunk = (feat, width)
    return pl.pallas_call(
        body,
        in_specs=[SMEM, SMEM, HBM, VMEM, VMEM, HBM, HBM, HBM],
        out_specs=[VMEM, VMEM, VMEM, HBM, HBM, VMEM, VMEM],
        out_shape=[
            in_vmem((rows, 2 * width), jnp.float32),
            in_vmem(chunk, jnp.bfloat16),
            in_vmem(chunk, jnp.bfloat16),
            in_hbm((rows, feat), jnp.bfloat16),
            in_hbm((rows, feat), jnp.bfloat16),
            in_vmem((w_out.shape[0], part), jnp.bfloat16),
            in_vmem((w_out.shape[0], part), jnp.bfloat16),
        ],
        scratch_shapes=[
            pltpu.VMEM((rows, feat), jnp.bfloat16),
            pltpu.VMEM((chunks - 1, 2, feat, width), jnp.bfloat16),
            pltpu.SemaphoreType.DMA((2 * chunks + 5,)),
        ],
        compiler_params=params(),
        cost_estimate=cost(12 * rows * feat * width, 20 * feat * width),
        name="project_near",
    )(where, core, *keep_in_hbm(own), left, right, *keep_in_hbm(w_key, w_value, w_out))


def project_last(asked, top, bottom, wk_last, wv_last, total):
    half, feat = top.shape
    rows = 2 * half
    width = wk_last.shape[1]
    peers = asked.shape[0]
    slots = peers * MOST

    def body(asked_hbm, t_ref, b_ref, wk, wv, tot_ref, pair_hbm, send_hbm, t_hbm, b_hbm, pick, pair, sem, sems, sends):
        get = pltpu.make_async_copy(asked_hbm, pick, sem)
        get.start()
        keep = [
            pltpu.make_async_copy(t_ref, t_hbm, sems.at[0]),
            pltpu.make_async_copy(b_ref, b_hbm, sems.at[1]),
        ]
        for copy in keep:
            copy.start()
        for j, w in enumerate((wk, wv)):
            cols = slice(j * width, (j + 1) * width)
            for lo, ref in ((0, t_ref), (half, b_ref)):
                span = slice(lo, lo + half)
                pair[span, cols] = (tot_ref[span, cols] + f32dot(ref[...], w[...])).astype(jnp.bfloat16)
            if j == 0:
                get.wait()
            for i in range(slots):
                block = jnp.clip(pick[i // MOST, i % MOST], 0, rows // BLK - 1)
                span = pl.ds(pl.multiple_of(block * BLK, BLK), BLK)
                pltpu.make_async_copy(pair.at[span, cols], send_hbm.at[i, :, cols], sends.at[j]).start()
        copy = pltpu.make_async_copy(pair, pair_hbm, sems.at[2])
        copy.start()
        keep.append(copy)
        for copy in keep:
            copy.wait()
        for j in range(2):
            sent = send_hbm.at[:, :, j * width : (j + 1) * width]
            pltpu.make_async_copy(sent, sent, sends.at[j]).wait()

    return pl.pallas_call(
        body,
        in_specs=[HBM, VMEM, VMEM, VMEM, VMEM, VMEM],
        out_specs=[HBM, HBM, HBM, HBM],
        out_shape=[
            in_hbm((rows, 2 * width), jnp.bfloat16),
            in_hbm((slots, BLK, 2 * width), jnp.bfloat16),
            in_hbm((half, feat), jnp.bfloat16),
            in_hbm((half, feat), jnp.bfloat16),
        ],
        scratch_shapes=[
            pltpu.SMEM((peers, HD), jnp.int32),
            pltpu.VMEM((rows, 2 * width), jnp.bfloat16),
            pltpu.SemaphoreType.DMA,
            pltpu.SemaphoreType.DMA((3,)),
            pltpu.SemaphoreType.DMA((2,)),
        ],
        compiler_params=params(),
        cost_estimate=cost(4 * rows * feat * width, 12 * feat * width),
        name="project_last",
    )(asked, top, bottom, wk_last, wv_last, total)


def project_query(where, own, left, right, top, bottom, w_query):
    rows, feat = own.shape
    half = top.shape[0]
    width = w_query.shape[1]

    def body(where_ref, o_ref, l_ref, r_ref, t_ref, b_ref, wo, wl, wr, wf, out_ref):
        for lo, far in ((0, t_ref), (half, b_ref)):
            span = slice(lo, lo + half)
            total = f32dot(o_ref[span, :], wo[...]) + f32dot(l_ref[span, :], wl[...])
            total = total + f32dot(r_ref[span, :], wr[...]) + f32dot(far[...], wf[...])
            out_ref[span, :] = total.astype(jnp.bfloat16)

    def chunk(k):
        return pl.BlockSpec((feat, width), lambda i, s: (s[k], 0))

    toks = pl.BlockSpec((rows, feat), lambda i, s: (0, 0))
    halves = pl.BlockSpec((half, feat), lambda i, s: (0, 0))
    return pl.pallas_call(
        body,
        grid_spec=pltpu.PrefetchScalarGridSpec(
            num_scalar_prefetch=1,
            grid=(1,),
            in_specs=[toks, toks, toks, halves, halves, chunk(0), chunk(1), chunk(2), chunk(3)],
            out_specs=pl.BlockSpec((rows, width), lambda i, s: (0, 0)),
        ),
        out_shape=in_vmem((rows, width), jnp.bfloat16),
        compiler_params=params(),
        cost_estimate=cost(8 * rows * feat * width, 16 * feat * width),
        name="project_query",
    )(where, *keep_in_hbm(own, left, right, top, bottom, w_query, w_query, w_query, w_query))


def plan(my_index, chosen, peers):
    rows, wide = chosen.shape
    slots = peers * MOST

    def body(me_ref, cho_ref, req_ref, mask_ref):
        me = me_ref[0]
        entries = cho_ref[...]
        peer = lax.broadcasted_iota(jnp.int32, (peers, wide), 0)
        low = jnp.full((peers, wide), rows, jnp.int32)
        high = jnp.full((peers, wide), -1, jnp.int32)
        for r in range(rows):
            entry = jnp.broadcast_to(entries[r : r + 1, :], (peers, wide))
            block = entry - peer * rows
            mine = (block >= 0) & (block < rows)
            low = jnp.where(mine, jnp.minimum(low, block), low)
            high = jnp.where(mine, jnp.maximum(high, block), high)
        low = jnp.min(low, axis=1, keepdims=True)
        high = jnp.max(high, axis=1, keepdims=True)
        far = lax.broadcasted_iota(jnp.int32, (peers, 1), 0) != me
        first = jnp.where(far & (low < rows), low, -1)
        second = jnp.where(far & (high > low), high, -1)
        lane = lax.broadcasted_iota(jnp.int32, (peers, HD), 1)
        req_ref[...] = jnp.where(lane == 0, first, jnp.where(lane == 1, second, -1))
        at = lax.broadcasted_iota(jnp.int32, (peers, HD), 0)
        named = jnp.where(lane == MOST * at, first, jnp.where(lane == MOST * at + 1, second, -1))
        named = jnp.where(named >= 0, named + at * rows, -1)
        ids = jnp.max(named, axis=0, keepdims=True)
        slot = lax.broadcasted_iota(jnp.int32, (1, HD), 1)
        own = (slot >= slots) & (slot < slots + rows)
        ids = jnp.where(own, me * rows + slot - slots, ids)
        seen = entries[:, :1] == ids
        for k in range(1, wide):
            seen = seen | (entries[:, k : k + 1] == ids)
        bias = jnp.where(seen, 0.0, NEG)
        for r in range(rows):
            mask_ref[r * BLK : (r + 1) * BLK, :] = jnp.broadcast_to(bias[r : r + 1, :], (BLK, HD)).astype(jnp.bfloat16)

    return pl.pallas_call(
        body,
        grid_spec=pltpu.PrefetchScalarGridSpec(
            num_scalar_prefetch=1,
            grid=(1,),
            in_specs=[pl.BlockSpec((rows, wide), lambda i, s: (0, 0))],
            out_specs=[
                pl.BlockSpec((peers, HD), lambda i, s: (0, 0)),
                pl.BlockSpec((rows * BLK, HD), lambda i, s: (0, 0)),
            ],
        ),
        out_shape=[in_hbm((peers, HD), jnp.int32), in_hbm((rows * BLK, HD), jnp.bfloat16)],
        compiler_params=params(),
        cost_estimate=cost(1000000, 200000),
        name="plan",
    )(my_index, chosen)


def one_hot(rows, first_slot):
    slot = lax.broadcasted_iota(jnp.int32, (rows, HD), 0) // BLK + first_slot
    return (slot == lax.broadcasted_iota(jnp.int32, (rows, HD), 1)).astype(jnp.bfloat16)


def scores_of(query, keys):
    return lax.dot_general(query, keys, (((1,), (1,)), ((), ())), preferred_element_type=jnp.float32)


def attend_own(query, pair, mask, first_slot):
    rows, width = query.shape
    heads = width // HD
    tile = 256

    def body(q_ref, k_ref, v_ref, mask_ref, sum_ref, log_ref):
        head = pl.program_id(0)
        keys = jnp.concatenate([k_ref[...], one_hot(rows, first_slot)], axis=1)
        values = jnp.concatenate([v_ref[...], jnp.ones_like(v_ref)], axis=1)
        for lo in range(0, rows, tile):
            span = slice(lo, lo + tile)
            count = lo + tile
            wide = jnp.concatenate([q_ref[span, :], mask_ref[span, :]], axis=1)
            scores = scores_of(wide, keys[:count])
            row = lax.broadcasted_iota(jnp.int32, scores.shape, 0) + lo
            col = lax.broadcasted_iota(jnp.int32, scores.shape, 1)
            scores = jnp.where(col <= row, scores, NEG)
            high = jnp.max(scores, axis=1, keepdims=True) * SCALE
            weights = jnp.exp2(scores * SCALE - high).astype(jnp.bfloat16)
            summed = f32dot(weights, values[:count])
            sum_ref[span, :] = summed[:, :HD] / summed[:, HD:]
            logs = high + jnp.log2(summed[:, HD:])
            lane = lax.broadcasted_iota(jnp.int32, logs.shape, 1)
            before = jnp.where(head == 0, 0.0, log_ref[span, :])
            log_ref[span, :] = jnp.where(lane == head, logs, before)

    column = pl.BlockSpec((rows, HD), lambda h: (0, h))
    narrow = pl.BlockSpec((rows, HD), lambda h: (0, 0))
    return pl.pallas_call(
        body,
        grid=(heads,),
        in_specs=[column, column, pl.BlockSpec((rows, HD), lambda h: (0, heads + h)), narrow],
        out_specs=[column, narrow],
        out_shape=[in_hbm((rows, width), jnp.float32), in_hbm((rows, HD), jnp.float32)],
        compiler_params=params(),
        cost_estimate=cost(8 * rows * rows * width, 16 * rows * width, rows * rows * heads),
        name="attend_own",
    )(query, *keep_in_hbm(pair, pair, mask))


def rows_for(where_ref, parts, tile):
    def rows_of(ref, cols=slice(None)):
        spans = [pl.ds(pl.multiple_of(where_ref[p] * tile, tile), tile) for p in parts]
        return jnp.concatenate([ref[span, cols] for span in spans], axis=0)

    return rows_of


def finished(scores, values, own, log):
    top = jnp.maximum(jnp.max(scores, axis=1, keepdims=True) * SCALE, log)
    weights = jnp.exp2(scores * SCALE - top).astype(jnp.bfloat16)
    far = f32dot(weights, values)
    keep = jnp.exp2(log - top)
    return ((far[:, :HD] + keep * own) / (far[:, HD:] + keep)).astype(jnp.bfloat16)


def attend_first(where, query, got, mask, own, log, parts):
    rows, width = query.shape
    heads = width // HD
    count = got.shape[0]
    tile = rows // where.shape[0]

    def body(where_ref, q_ref, got_ref, mask_hbm, own_hbm, log_hbm, out_a, out_b, keys, values, mask, own, log, sems):
        copies = [
            pltpu.make_async_copy(src, dst, sems.at[k])
            for k, (src, dst) in enumerate(((mask_hbm, mask), (own_hbm, own), (log_hbm, log)))
        ]
        for copy in copies:
            copy.start()
        hot = one_hot(count, 0)
        rows_of = rows_for(where_ref, parts, tile)

        def scores_at(h):
            keys[h, :, :HD] = got_ref[:, h * HD : (h + 1) * HD]
            keys[h, :, HD:] = hot
            if h == 0:
                copies[0].wait()
            query = rows_of(q_ref, slice(h * HD, (h + 1) * HD))
            return scores_of(jnp.concatenate([query, rows_of(mask)], axis=1), keys[h])

        later = scores_at(0)
        for h in range(heads):
            scores = later
            values[h, :, :HD] = got_ref[:, (heads + h) * HD : (heads + h + 1) * HD]
            values[h, :, HD:] = jnp.ones((count, HD), jnp.bfloat16)
            if h + 1 < heads:
                later = scores_at(h + 1)
            if h == 0:
                copies[1].wait()
                copies[2].wait()
            cols = slice(h * HD, (h + 1) * HD)
            result = finished(scores, values[h], rows_of(own, cols), rows_of(log)[:, h : h + 1])
            out_a[:, cols] = result[:tile]
            out_b[:, cols] = result[tile:]

    wides = in_vmem((heads, count, 2 * HD), jnp.bfloat16)
    return pl.pallas_call(
        body,
        in_specs=[SMEM, VMEM, VMEM, HBM, HBM, HBM],
        out_specs=[VMEM] * 7,
        out_shape=[in_vmem((tile, width), jnp.bfloat16)] * 2
        + [wides] * 2
        + [
            in_vmem(mask.shape, jnp.bfloat16),
            in_vmem(own.shape, jnp.float32),
            in_vmem(log.shape, jnp.float32),
        ],
        scratch_shapes=[pltpu.SemaphoreType.DMA((3,))],
        compiler_params=params(),
        cost_estimate=cost(4 * rows * count * width, 4 * count * width, rows * count * heads),
        name="attend_first",
    )(where, query, got, *keep_in_hbm(mask, own, log))


def attend_second(where, query, keys, values, mask, own, log, parts, carried):
    rows, width = query.shape
    heads, count, _ = keys.shape
    tile = rows // where.shape[0]
    pieces = len(carried)

    def body(where_ref, q_ref, keys_ref, values_ref, mask_ref, own_ref, log_ref, *rest):
        out_a, out_b = rest[pieces : pieces + 2]
        copies = [pltpu.make_async_copy(rest[k], rest[pieces + 2 + k], rest[-1].at[k]) for k in range(pieces)]
        for copy in copies:
            copy.start()
        rows_of = rows_for(where_ref, parts, tile)

        def scores_at(h):
            query = rows_of(q_ref, slice(h * HD, (h + 1) * HD))
            return scores_of(jnp.concatenate([query, rows_of(mask_ref)], axis=1), keys_ref[h])

        later = scores_at(0)
        for h in range(heads):
            scores = later
            if h + 1 < heads:
                later = scores_at(h + 1)
            cols = slice(h * HD, (h + 1) * HD)
            result = finished(scores, values_ref[h], rows_of(own_ref, cols), rows_of(log_ref)[:, h : h + 1])
            out_a[:, cols] = result[:tile]
            out_b[:, cols] = result[tile:]
        for copy in copies:
            copy.wait()

    return pl.pallas_call(
        body,
        in_specs=[SMEM] + [VMEM] * 6 + [HBM] * pieces,
        out_specs=[VMEM] * (2 + pieces),
        out_shape=[in_vmem((tile, width), jnp.bfloat16)] * 2 + [in_vmem(w.shape, w.dtype) for w in carried],
        scratch_shapes=[pltpu.SemaphoreType.DMA((pieces,))],
        compiler_params=params(),
        cost_estimate=cost(4 * rows * count * width, 4 * count * width, rows * count * heads),
        name="attend_second",
    )(where, query, keys, values, mask, own, log, *keep_in_hbm(*carried))


def mix_near(core, attended, w_own, mine, other):
    rows = attended[0].shape[0]
    part = mine[0].shape[1]

    def body(core_ref, own_ref, right_ref, far_ref, w_ref, *rest):
        out_ref = rest[-1]
        for side, pieces in enumerate((rest[:4], rest[4:8])):
            base = (core_ref[0] if side == 0 else 1 - core_ref[0]) * 2
            for k in range(2):
                span = pl.ds(pl.multiple_of((base + k) * part, part), part)
                total = f32dot(own_ref[...], w_ref[:, span]) + f32dot(right_ref[...], pieces[k][...])
                out_ref[:, span] = total + f32dot(far_ref[...], pieces[2 + k][...])

    args = (*attended, w_own, *mine, *other)
    return pl.pallas_call(
        body,
        in_specs=[SMEM] + [VMEM] * len(args),
        out_specs=VMEM,
        out_shape=in_vmem((rows, 4 * part), jnp.float32),
        compiler_params=params(),
        cost_estimate=cost(24 * rows * w_own.shape[0] * part, 24 * w_own.shape[0] * part),
        name="mix_near",
    )(core, *args)


def mix_last(core, left, mine, other, before):
    rows = left.shape[0]
    part = mine[0].shape[1]

    def body(core_ref, left_ref, *rest):
        before_ref, out_hbm, out_ref, sems = rest[4:]
        copies = []
        for at in range(4):
            base = (core_ref[0] if at < 2 else 1 - core_ref[0]) * 2
            span = pl.ds(pl.multiple_of((base + at % 2) * part, part), part)
            out_ref[at] = (before_ref[:, span] + f32dot(left_ref[...], rest[at][...])).astype(jnp.bfloat16)
            copies.append(pltpu.make_async_copy(out_ref.at[at], out_hbm.at[:, span], sems.at[at]))
            copies[-1].start()
        for copy in copies:
            copy.wait()

    return pl.pallas_call(
        body,
        in_specs=[SMEM] + [VMEM] * 6,
        out_specs=HBM,
        out_shape=in_hbm((rows, 4 * part), jnp.bfloat16),
        scratch_shapes=[pltpu.VMEM((4, rows, part), jnp.bfloat16), pltpu.SemaphoreType.DMA((4,))],
        compiler_params=params(),
        cost_estimate=cost(8 * rows * left.shape[1] * part, 8 * left.shape[1] * part),
        name="mix_last",
    )(core, left, *mine, *other, before)


def local(tokens, w_query, w_key, w_value, w_out, chosen):
    tok_rows = tokens.shape[0]
    width = w_query.shape[1]
    half = tok_rows // 2
    peers = lax.axis_size(KV)
    tp = lax.axis_index("tp")
    count = lax.axis_size("tp")
    where = jnp.stack([tp, (tp + count - 1) % count, (tp + 1) % count, (tp + 2) % count]).astype(jnp.int32)
    me = jnp.reshape(lax.axis_index(KV), (1,)).astype(jnp.int32)
    core = jnp.reshape(lax.axis_index("kv_2"), (1,)).astype(jnp.int32)
    tokens, where, me, core = lax.optimization_barrier((tokens, where, me, core))

    left = shifted(tokens, "tp", 1)
    right = shifted(tokens, "tp", -1)
    request, mask = plan(me, chosen, peers)
    asked = lax.all_to_all(request, KV, 0, 0, tiled=True)
    left, right, request, mask = lax.optimization_barrier((left, right, request, mask))

    top = shifted(left[:half], "tp", 1)
    bottom = shifted(right[half:], "tp", -1)
    total, wk_last, wv_last, left, right, low, high_part = project_near(
        where, core, tokens, left, right, w_key, w_value, w_out
    )
    pair, send, top, bottom = project_last(asked, top, bottom, wk_last, wv_last, total)
    low, high_part, send = lax.optimization_barrier((low, high_part, send))
    got = lax.all_to_all(send, KV, split_axis=0, concat_axis=0, tiled=True)

    left_low = shifted(low, "tp", 1)
    right_high = shifted(high_part, "tp", -1)
    left_high = shifted(high_part, "tp", 1)
    right_low = shifted(low, "tp", -1)
    far_low = shifted(left_low, "tp", 1)
    far_high = shifted(right_high, "tp", -1)
    mine = (left_low, left_high, right_low, right_high, far_low, far_high)
    other = tuple(shifted(w, "kv_2", 1) for w in mine)

    query = project_query(where, tokens, left, right, top, bottom, w_query)
    own, log = attend_own(query, pair, mask, peers * MOST)
    to_far, to_left, keys, values, mask, own, log = attend_first(
        where, query, got.reshape(-1, 2 * width), mask, own, log, (3, 1)
    )
    far = shifted(to_far, "tp", 2)
    right = shifted(to_left, "tp", -1)
    carried = (w_out, *mine, *other)
    to_right, mid, w_own, *pieces = attend_second(where, query, keys, values, mask, own, log, (2, 0), carried)
    left = shifted(to_right, "tp", 1)
    mine, other = pieces[:6], pieces[6:]
    before = mix_near(core, (mid, right, far), w_own, mine[2:], other[2:])
    return mix_last(core, left, mine[:2], other[:2], before)


def solution(mesh):
    finer = Mesh(mesh.devices.reshape(4, 4, 2, mesh.shape["tp"]), ("kv_0", "kv_1", "kv_2", "tp"))
    placed = (P(KV, "tp"), P(None, "tp"), P(None, "tp"), P(None, "tp"), P("tp", None), P(KV, None))

    return jax.shard_map(local, mesh=finer, in_specs=placed, out_specs=P(KV_TP, None), check_vma=False)
```

```python
import jax
import jax.numpy as jnp
from jax import lax
from jax.experimental import pallas as pl
from jax.experimental.pallas import tpu as pltpu
from jax.sharding import Mesh
from jax.sharding import PartitionSpec as P


HD = 128
BLK = 32
MOST = 2
KV = ("kv_0", "kv_1", "kv_2")
KV_TP = ("kv_0", "kv_1", "kv_2", "tp")
NEG = -1e30
SCALE = HD ** (-0.5) * 1.4426950408889634
SMALL = 24 * 1024 * 1024
HBM = pl.BlockSpec(memory_space=pltpu.HBM)
VMEM = pl.BlockSpec(memory_space=pltpu.VMEM)
SMEM = pl.BlockSpec(memory_space=pltpu.SMEM)


def params(limit=SMALL):
    return pltpu.CompilerParams(vmem_limit_bytes=limit)


def in_hbm(shape, dtype):
    return pltpu.HBM(shape, dtype)


def in_vmem(shape, dtype):
    return pltpu.VMEM(shape, dtype)


def cost(flops, nbytes, exps=0):
    return pl.CostEstimate(flops=int(flops), bytes_accessed=int(nbytes), transcendentals=int(exps))


def keep_in_hbm(*arrays):
    return tuple(pltpu.with_memory_space_constraint(a, pltpu.HBM) for a in arrays)


def f32dot(a, b):
    return jnp.dot(a, b, preferred_element_type=jnp.float32)


def shifted(array, axis, by):
    count = lax.axis_size(axis)
    return lax.ppermute(array, axis, [(i, (i + by) % count) for i in range(count)])


def project_near(where, core, own, left, right, w_key, w_value, w_out):
    rows, feat = own.shape
    width = w_key.shape[1]
    chunks = where.shape[0]
    part = w_out.shape[1] // 4

    def body(where_ref, core_ref, own_hbm, l_ref, r_ref, wk_hbm, wv_hbm, w_hbm, *rest):
        tot_ref, wk_last, wv_last, l_hbm, r_hbm, low_ref, high_ref, own_ref, chunk_refs, sems = rest
        copies = []

        def fetch(src, dst):
            copies.append(pltpu.make_async_copy(src, dst, sems.at[len(copies)]))
            copies[-1].start()
            return copies[-1]

        own_copy = fetch(own_hbm, own_ref)
        pieces = []
        for k in range(chunks - 1):
            span = pl.ds(pl.multiple_of(where_ref[k] * feat, feat), feat)
            for j, w in enumerate((wk_hbm, wv_hbm)):
                pieces.append(fetch(w.at[span, :], chunk_refs.at[k, j]))
        span = pl.ds(pl.multiple_of(where_ref[chunks - 1] * feat, feat), feat)
        last = [fetch(wk_hbm.at[span, :], wk_last), fetch(wv_hbm.at[span, :], wv_last)]
        last += [fetch(l_ref, l_hbm), fetch(r_ref, r_hbm)]
        for k, ref in enumerate((low_ref, high_ref)):
            at = pl.multiple_of((2 * core_ref[0] + k) * part, part)
            last.append(fetch(w_hbm.at[:, pl.ds(at, part)], ref))
        own_copy.wait()
        for copy in pieces:
            copy.wait()
        for j in range(2):
            total = f32dot(own_ref[...], chunk_refs[0, j]) + f32dot(l_ref[...], chunk_refs[1, j])
            tot_ref[:, j * width : (j + 1) * width] = total + f32dot(r_ref[...], chunk_refs[2, j])
        for copy in last:
            copy.wait()

    chunk = (feat, width)
    return pl.pallas_call(
        body,
        in_specs=[SMEM, SMEM, HBM, VMEM, VMEM, HBM, HBM, HBM],
        out_specs=[VMEM, VMEM, VMEM, HBM, HBM, VMEM, VMEM],
        out_shape=[
            in_vmem((rows, 2 * width), jnp.float32),
            in_vmem(chunk, jnp.bfloat16),
            in_vmem(chunk, jnp.bfloat16),
            in_hbm((rows, feat), jnp.bfloat16),
            in_hbm((rows, feat), jnp.bfloat16),
            in_vmem((w_out.shape[0], part), jnp.bfloat16),
            in_vmem((w_out.shape[0], part), jnp.bfloat16),
        ],
        scratch_shapes=[
            pltpu.VMEM((rows, feat), jnp.bfloat16),
            pltpu.VMEM((chunks - 1, 2, feat, width), jnp.bfloat16),
            pltpu.SemaphoreType.DMA((2 * chunks + 5,)),
        ],
        compiler_params=params(),
        cost_estimate=cost(12 * rows * feat * width, 20 * feat * width),
        name="project_near",
    )(where, core, *keep_in_hbm(own), left, right, *keep_in_hbm(w_key, w_value, w_out))


def project_last(asked, top, bottom, wk_last, wv_last, total):
    half, feat = top.shape
    rows = 2 * half
    width = wk_last.shape[1]
    peers = asked.shape[0]
    slots = peers * MOST

    def body(asked_hbm, t_ref, b_ref, wk, wv, tot_ref, pair_hbm, send_hbm, t_hbm, b_hbm, pick, pair, sem, sems, sends):
        get = pltpu.make_async_copy(asked_hbm, pick, sem)
        get.start()
        keep = [
            pltpu.make_async_copy(t_ref, t_hbm, sems.at[0]),
            pltpu.make_async_copy(b_ref, b_hbm, sems.at[1]),
        ]
        for copy in keep:
            copy.start()
        for j, w in enumerate((wk, wv)):
            cols = slice(j * width, (j + 1) * width)
            for lo, ref in ((0, t_ref), (half, b_ref)):
                span = slice(lo, lo + half)
                pair[span, cols] = (tot_ref[span, cols] + f32dot(ref[...], w[...])).astype(jnp.bfloat16)
            if j == 0:
                get.wait()
            for i in range(slots):
                block = jnp.clip(pick[i // MOST, i % MOST], 0, rows // BLK - 1)
                span = pl.ds(pl.multiple_of(block * BLK, BLK), BLK)
                pltpu.make_async_copy(pair.at[span, cols], send_hbm.at[i, :, cols], sends.at[j]).start()
        copy = pltpu.make_async_copy(pair, pair_hbm, sems.at[2])
        copy.start()
        keep.append(copy)
        for copy in keep:
            copy.wait()
        for j in range(2):
            sent = send_hbm.at[:, :, j * width : (j + 1) * width]
            pltpu.make_async_copy(sent, sent, sends.at[j]).wait()

    return pl.pallas_call(
        body,
        in_specs=[HBM, VMEM, VMEM, VMEM, VMEM, VMEM],
        out_specs=[HBM, HBM, HBM, HBM],
        out_shape=[
            in_hbm((rows, 2 * width), jnp.bfloat16),
            in_hbm((slots, BLK, 2 * width), jnp.bfloat16),
            in_hbm((half, feat), jnp.bfloat16),
            in_hbm((half, feat), jnp.bfloat16),
        ],
        scratch_shapes=[
            pltpu.SMEM((peers, HD), jnp.int32),
            pltpu.VMEM((rows, 2 * width), jnp.bfloat16),
            pltpu.SemaphoreType.DMA,
            pltpu.SemaphoreType.DMA((3,)),
            pltpu.SemaphoreType.DMA((2,)),
        ],
        compiler_params=params(),
        cost_estimate=cost(4 * rows * feat * width, 12 * feat * width),
        name="project_last",
    )(asked, top, bottom, wk_last, wv_last, total)


def project_query(where, own, left, right, top, bottom, w_query):
    rows, feat = own.shape
    half = top.shape[0]
    width = w_query.shape[1]

    def body(where_ref, o_ref, l_ref, r_ref, t_ref, b_ref, wo, wl, wr, wf, out_ref):
        for lo, far in ((0, t_ref), (half, b_ref)):
            span = slice(lo, lo + half)
            total = f32dot(o_ref[span, :], wo[...]) + f32dot(l_ref[span, :], wl[...])
            total = total + f32dot(r_ref[span, :], wr[...]) + f32dot(far[...], wf[...])
            out_ref[span, :] = total.astype(jnp.bfloat16)

    def chunk(k):
        return pl.BlockSpec((feat, width), lambda i, s: (s[k], 0))

    toks = pl.BlockSpec((rows, feat), lambda i, s: (0, 0))
    halves = pl.BlockSpec((half, feat), lambda i, s: (0, 0))
    return pl.pallas_call(
        body,
        grid_spec=pltpu.PrefetchScalarGridSpec(
            num_scalar_prefetch=1,
            grid=(1,),
            in_specs=[toks, toks, toks, halves, halves, chunk(0), chunk(1), chunk(2), chunk(3)],
            out_specs=pl.BlockSpec((rows, width), lambda i, s: (0, 0)),
        ),
        out_shape=in_vmem((rows, width), jnp.bfloat16),
        compiler_params=params(),
        cost_estimate=cost(8 * rows * feat * width, 16 * feat * width),
        name="project_query",
    )(where, *keep_in_hbm(own, left, right, top, bottom, w_query, w_query, w_query, w_query))


def plan(my_index, chosen, peers):
    rows, wide = chosen.shape
    slots = peers * MOST

    def body(me_ref, cho_ref, req_ref, mask_ref):
        me = me_ref[0]
        entries = cho_ref[...]
        peer = lax.broadcasted_iota(jnp.int32, (peers, wide), 0)
        low = jnp.full((peers, wide), rows, jnp.int32)
        high = jnp.full((peers, wide), -1, jnp.int32)
        for r in range(rows):
            entry = jnp.broadcast_to(entries[r : r + 1, :], (peers, wide))
            block = entry - peer * rows
            mine = (block >= 0) & (block < rows)
            low = jnp.where(mine, jnp.minimum(low, block), low)
            high = jnp.where(mine, jnp.maximum(high, block), high)
        low = jnp.min(low, axis=1, keepdims=True)
        high = jnp.max(high, axis=1, keepdims=True)
        far = lax.broadcasted_iota(jnp.int32, (peers, 1), 0) != me
        first = jnp.where(far & (low < rows), low, -1)
        second = jnp.where(far & (high > low), high, -1)
        lane = lax.broadcasted_iota(jnp.int32, (peers, HD), 1)
        req_ref[...] = jnp.where(lane == 0, first, jnp.where(lane == 1, second, -1))
        at = lax.broadcasted_iota(jnp.int32, (peers, HD), 0)
        named = jnp.where(lane == MOST * at, first, jnp.where(lane == MOST * at + 1, second, -1))
        named = jnp.where(named >= 0, named + at * rows, -1)
        ids = jnp.max(named, axis=0, keepdims=True)
        slot = lax.broadcasted_iota(jnp.int32, (1, HD), 1)
        own = (slot >= slots) & (slot < slots + rows)
        ids = jnp.where(own, me * rows + slot - slots, ids)
        seen = entries[:, :1] == ids
        for k in range(1, wide):
            seen = seen | (entries[:, k : k + 1] == ids)
        bias = jnp.where(seen, 0.0, NEG)
        for r in range(rows):
            mask_ref[r * BLK : (r + 1) * BLK, :] = jnp.broadcast_to(bias[r : r + 1, :], (BLK, HD)).astype(jnp.bfloat16)

    return pl.pallas_call(
        body,
        grid_spec=pltpu.PrefetchScalarGridSpec(
            num_scalar_prefetch=1,
            grid=(1,),
            in_specs=[pl.BlockSpec((rows, wide), lambda i, s: (0, 0))],
            out_specs=[
                pl.BlockSpec((peers, HD), lambda i, s: (0, 0)),
                pl.BlockSpec((rows * BLK, HD), lambda i, s: (0, 0)),
            ],
        ),
        out_shape=[in_hbm((peers, HD), jnp.int32), in_hbm((rows * BLK, HD), jnp.bfloat16)],
        compiler_params=params(),
        cost_estimate=cost(1000000, 200000),
        name="plan",
    )(my_index, chosen)


def one_hot(rows, first_slot):
    slot = lax.broadcasted_iota(jnp.int32, (rows, HD), 0) // BLK + first_slot
    return (slot == lax.broadcasted_iota(jnp.int32, (rows, HD), 1)).astype(jnp.bfloat16)


def scores_of(query, keys):
    return lax.dot_general(query, keys, (((1,), (1,)), ((), ())), preferred_element_type=jnp.float32)


def attend_own(query, pair, mask, first_slot):
    rows, width = query.shape
    heads = width // HD
    tile = 256

    def body(q_ref, k_ref, v_ref, mask_ref, sum_ref, log_ref):
        head = pl.program_id(0)
        keys = jnp.concatenate([k_ref[...], one_hot(rows, first_slot)], axis=1)
        values = jnp.concatenate([v_ref[...], jnp.ones_like(v_ref)], axis=1)
        for lo in range(0, rows, tile):
            span = slice(lo, lo + tile)
            count = lo + tile
            wide = jnp.concatenate([q_ref[span, :], mask_ref[span, :]], axis=1)
            scores = scores_of(wide, keys[:count])
            row = lax.broadcasted_iota(jnp.int32, scores.shape, 0) + lo
            col = lax.broadcasted_iota(jnp.int32, scores.shape, 1)
            scores = jnp.where(col <= row, scores, NEG)
            high = jnp.max(scores, axis=1, keepdims=True) * SCALE
            weights = jnp.exp2(scores * SCALE - high).astype(jnp.bfloat16)
            summed = f32dot(weights, values[:count])
            sum_ref[span, :] = summed[:, :HD] / summed[:, HD:]
            logs = high + jnp.log2(summed[:, HD:])
            lane = lax.broadcasted_iota(jnp.int32, logs.shape, 1)
            before = jnp.where(head == 0, 0.0, log_ref[span, :])
            log_ref[span, :] = jnp.where(lane == head, logs, before)

    column = pl.BlockSpec((rows, HD), lambda h: (0, h))
    narrow = pl.BlockSpec((rows, HD), lambda h: (0, 0))
    return pl.pallas_call(
        body,
        grid=(heads,),
        in_specs=[column, column, pl.BlockSpec((rows, HD), lambda h: (0, heads + h)), narrow],
        out_specs=[column, narrow],
        out_shape=[in_hbm((rows, width), jnp.float32), in_hbm((rows, HD), jnp.float32)],
        compiler_params=params(),
        cost_estimate=cost(8 * rows * rows * width, 16 * rows * width, rows * rows * heads),
        name="attend_own",
    )(query, *keep_in_hbm(pair, pair, mask))


def rows_for(where_ref, parts, tile):
    def rows_of(ref, cols=slice(None)):
        spans = [pl.ds(pl.multiple_of(where_ref[p] * tile, tile), tile) for p in parts]
        return jnp.concatenate([ref[span, cols] for span in spans], axis=0)

    return rows_of


def finished(scores, values, own, log):
    top = jnp.maximum(jnp.max(scores, axis=1, keepdims=True) * SCALE, log)
    weights = jnp.exp2(scores * SCALE - top).astype(jnp.bfloat16)
    far = f32dot(weights, values)
    keep = jnp.exp2(log - top)
    return ((far[:, :HD] + keep * own) / (far[:, HD:] + keep)).astype(jnp.bfloat16)


def attend_first(where, query, got, mask, own, log, groups):
    rows, width = query.shape
    heads = width // HD
    count = got.shape[0]
    tile = rows // where.shape[0]
    places = [part for group in groups for part in group]
    outs = len(places)

    def body(where_ref, q_ref, got_ref, mask_hbm, own_hbm, log_hbm, *rest):
        keys, values, mask, own, log, sems = rest[outs:]
        copies = [
            pltpu.make_async_copy(src, dst, sems.at[k])
            for k, (src, dst) in enumerate(((mask_hbm, mask), (own_hbm, own), (log_hbm, log)))
        ]
        for copy in copies:
            copy.start()
        hot = one_hot(count, 0)
        steps = [(h, group) for h in range(heads) for group in groups]

        def scores_at(i):
            h, group = steps[i]
            if i % len(groups) == 0:
                keys[h, :, :HD] = got_ref[:, h * HD : (h + 1) * HD]
                keys[h, :, HD:] = hot
            if i == 0:
                copies[0].wait()
            rows_of = rows_for(where_ref, group, tile)
            query = rows_of(q_ref, slice(h * HD, (h + 1) * HD))
            return scores_of(jnp.concatenate([query, rows_of(mask)], axis=1), keys[h])

        later = scores_at(0)
        for i, (h, group) in enumerate(steps):
            scores = later
            if i % len(groups) == 0:
                values[h, :, :HD] = got_ref[:, (heads + h) * HD : (heads + h + 1) * HD]
                values[h, :, HD:] = jnp.ones((count, HD), jnp.bfloat16)
            if i + 1 < len(steps):
                later = scores_at(i + 1)
            if i == 0:
                copies[1].wait()
                copies[2].wait()
            cols = slice(h * HD, (h + 1) * HD)
            rows_of = rows_for(where_ref, group, tile)
            result = finished(scores, values[h], rows_of(own, cols), rows_of(log)[:, h : h + 1])
            for k, part in enumerate(group):
                rest[places.index(part)][:, cols] = result[k * tile : (k + 1) * tile]

    wides = in_vmem((heads, count, 2 * HD), jnp.bfloat16)
    return pl.pallas_call(
        body,
        in_specs=[SMEM, VMEM, VMEM, HBM, HBM, HBM],
        out_specs=[VMEM] * (outs + 5),
        out_shape=[in_vmem((tile, width), jnp.bfloat16)] * outs
        + [wides] * 2
        + [
            in_vmem(mask.shape, jnp.bfloat16),
            in_vmem(own.shape, jnp.float32),
            in_vmem(log.shape, jnp.float32),
        ],
        scratch_shapes=[pltpu.SemaphoreType.DMA((3,))],
        compiler_params=params(),
        cost_estimate=cost(6 * rows * count * width, 4 * count * width, rows * count * heads),
        name="attend_first",
    )(where, query, got, *keep_in_hbm(mask, own, log))


def attend_second(where, query, keys, values, mask, own, log, carried):
    rows, width = query.shape
    heads, count, _ = keys.shape
    tile = rows // where.shape[0]
    pieces = len(carried)

    def body(where_ref, q_ref, keys_ref, values_ref, mask_ref, own_ref, log_ref, *rest):
        out_ref = rest[pieces]
        copies = [pltpu.make_async_copy(rest[k], rest[pieces + 1 + k], rest[-1].at[k]) for k in range(pieces)]
        for copy in copies:
            copy.start()
        rows_of = rows_for(where_ref, (0,), tile)

        def scores_at(h):
            query = rows_of(q_ref, slice(h * HD, (h + 1) * HD))
            return scores_of(jnp.concatenate([query, rows_of(mask_ref)], axis=1), keys_ref[h])

        later = scores_at(0)
        for h in range(heads):
            scores = later
            if h + 1 < heads:
                later = scores_at(h + 1)
            cols = slice(h * HD, (h + 1) * HD)
            out_ref[:, cols] = finished(
                scores, values_ref[h], rows_of(own_ref, cols), rows_of(log_ref)[:, h : h + 1]
            )
        for copy in copies:
            copy.wait()

    return pl.pallas_call(
        body,
        in_specs=[SMEM] + [VMEM] * 6 + [HBM] * pieces,
        out_specs=[VMEM] * (1 + pieces),
        out_shape=[in_vmem((tile, width), jnp.bfloat16)] + [in_vmem(w.shape, w.dtype) for w in carried],
        scratch_shapes=[pltpu.SemaphoreType.DMA((pieces,))],
        compiler_params=params(),
        cost_estimate=cost(2 * rows * count * width, 4 * count * width, rows * count * heads),
        name="attend_second",
    )(where, query, keys, values, mask, own, log, *keep_in_hbm(*carried))


def mix(core, attended, w_own, mine, other):
    rows, width = attended[0].shape
    part = mine[0].shape[1]

    def body(core_ref, *rest):
        own_ref, far_refs, w_ref, pieces = rest[0], rest[1:4], rest[4], (rest[5:11], rest[11:17])
        out_hbm, out_ref, sems = rest[17:]
        copies = []
        for side in range(2):
            base = (core_ref[0] if side == 0 else 1 - core_ref[0]) * 2
            for k in range(2):
                span = pl.ds(pl.multiple_of((base + k) * part, part), part)
                total = f32dot(own_ref[...], w_ref[:, span])
                for g in range(3):
                    total = total + f32dot(far_refs[g][...], pieces[side][2 * g + k][...])
                at = 2 * side + k
                out_ref[at] = total.astype(jnp.bfloat16)
                copies.append(pltpu.make_async_copy(out_ref.at[at], out_hbm.at[:, span], sems.at[at]))
                copies[-1].start()
        for copy in copies:
            copy.wait()

    args = (*attended, w_own, *mine, *other)
    return pl.pallas_call(
        body,
        in_specs=[SMEM] + [VMEM] * len(args),
        out_specs=HBM,
        out_shape=in_hbm((rows, 4 * part), jnp.bfloat16),
        scratch_shapes=[pltpu.VMEM((4, rows, part), jnp.bfloat16), pltpu.SemaphoreType.DMA((4,))],
        compiler_params=params(),
        cost_estimate=cost(32 * rows * width * part, 32 * width * part),
        name="mix",
    )(core, *args)


def local(tokens, w_query, w_key, w_value, w_out, chosen):
    tok_rows = tokens.shape[0]
    width = w_query.shape[1]
    half = tok_rows // 2
    peers = lax.axis_size(KV)
    tp = lax.axis_index("tp")
    count = lax.axis_size("tp")
    where = jnp.stack([tp, (tp + count - 1) % count, (tp + 1) % count, (tp + 2) % count]).astype(jnp.int32)
    me = jnp.reshape(lax.axis_index(KV), (1,)).astype(jnp.int32)
    core = jnp.reshape(lax.axis_index("kv_2"), (1,)).astype(jnp.int32)
    tokens, where, me, core = lax.optimization_barrier((tokens, where, me, core))

    left = shifted(tokens, "tp", 1)
    right = shifted(tokens, "tp", -1)
    request, mask = plan(me, chosen, peers)
    asked = lax.all_to_all(request, KV, 0, 0, tiled=True)
    left, right, request, mask = lax.optimization_barrier((left, right, request, mask))

    top = shifted(left[:half], "tp", 1)
    bottom = shifted(right[half:], "tp", -1)
    total, wk_last, wv_last, left, right, low, high_part = project_near(
        where, core, tokens, left, right, w_key, w_value, w_out
    )
    pair, send, top, bottom = project_last(asked, top, bottom, wk_last, wv_last, total)
    low, high_part, send = lax.optimization_barrier((low, high_part, send))
    got = lax.all_to_all(send, KV, split_axis=0, concat_axis=0, tiled=True)

    left_low = shifted(low, "tp", 1)
    right_high = shifted(high_part, "tp", -1)
    left_high = shifted(high_part, "tp", 1)
    right_low = shifted(low, "tp", -1)
    far_low = shifted(left_low, "tp", 1)
    far_high = shifted(right_high, "tp", -1)
    mine = (left_low, left_high, right_low, right_high, far_low, far_high)
    other = tuple(shifted(w, "kv_2", 1) for w in mine)

    query = project_query(where, tokens, left, right, top, bottom, w_query)
    own, log = attend_own(query, pair, mask, peers * MOST)
    to_far, to_left, to_right, keys, values, mask, own, log = attend_first(
        where, query, got.reshape(-1, 2 * width), mask, own, log, ((3, 1), (2,))
    )
    far = shifted(to_far, "tp", 2)
    right = shifted(to_left, "tp", -1)
    left = shifted(to_right, "tp", 1)
    carried = (w_out, *mine, *other)
    mid, w_own, *pieces = attend_second(where, query, keys, values, mask, own, log, carried)
    return mix(core, (mid, left, right, far), w_own, pieces[:6], pieces[6:])


def solution(mesh):
    finer = Mesh(mesh.devices.reshape(4, 4, 2, mesh.shape["tp"]), ("kv_0", "kv_1", "kv_2", "tp"))
    placed = (P(KV, "tp"), P(None, "tp"), P(None, "tp"), P(None, "tp"), P("tp", None), P(KV, None))

    return jax.shard_map(local, mesh=finer, in_specs=placed, out_specs=P(KV_TP, None), check_vma=False)
```
